32 devices in a mesh: sp: 8 (over z, y), tp: 4 (over x, core).
Axes of the slice: x: 2, y: 2, z: 4, core: 2. Of those that a mesh axis runs over, the one named last changes fastest.
Arguments:
- cotangent: bfloat16 [1280, 2048], P('sp'), may hold values from -8 to 8
- saved_input: bfloat16 [1280, 2048], P('sp'), may hold values from -200 to 200
- routes: int32 [1280, 2], P('sp'), may hold values from 0 to 7, all different within a row; in each aligned block of 160 rows (0 to 159, 160 to 319, ...) at most 80 rows name the same one
- route_weight: float32 [1280, 2], P('sp'), may hold values from 0.2 to 1.5
- gate_proj: bfloat16 [8, 2048, 1024], P('sp', None, 'tp'), may hold values from -0.125 to 0.125
- up_proj: bfloat16 [8, 2048, 1024], P('sp', None, 'tp'), may hold values from -0.125 to 0.125
- down_proj: bfloat16 [8, 1024, 2048], P('sp', 'tp'), may hold values from -0.1875 to 0.1875
- out_proj: bfloat16 [2048, 1024], P(None, 'tp'), may hold values from -0.1875 to 0.1875
- conv_input: bfloat16 [1280, 1024], P('sp', 'tp'), may hold values from -6 to 6
- gate_branch: bfloat16 [1280, 1024], P('sp', 'tp'), may hold values from -6 to 6
- conv_taps: bfloat16 [4, 1024], P(None, 'tp'), may hold values from -3 to 3
- recur_map: bfloat16 [2, 16, 64, 64], P(None, 'tp'), may hold values from -0.75 to 0.75
- input_map: bfloat16 [2, 16, 64, 64], P(None, 'tp'), may hold values from -0.75 to 0.75
- decay_param: float32 [2, 1024], P(None, 'tp'), may hold values from 4 to 30
- decay_shift: float32 [2, 1280, 1024], P(None, 'sp', 'tp'), may hold values from -2 to 0, as said below
Outputs:
- grad_gate_proj: float32 [8, 2048, 1024], P('sp', None, 'tp')
- grad_up_proj: float32 [8, 2048, 1024], P('sp', None, 'tp')
- grad_down_proj: float32 [8, 1024, 2048], P('sp', 'tp')
- grad_out_proj: float32 [2048, 1024], P('sp', 'tp')
- grad_conv_input: bfloat16 [1280, 1024], P('sp', 'tp')
- grad_gate_branch: bfloat16 [1280, 1024], P('sp', 'tp')
The draws below stay inside these ranges and needn't reach their ends.
Inputs may be any that keep to these rules, and one draw needn't show every extreme that they name: Each row names 2 different experts; among the rows of one device no expert is named by more than 80 rows, and in every draw some device routes exactly 80 rows to some expert. `decay_shift`: together with decay_param, -log_decay stays at or above softplus(-decay_param) for every channel and position.
All inputs are finite; a program needn't handle non-finite values.
Results may differ from the reference program's by a relative error of at most 0.013.
Values may be sent and summed in bfloat16 or wider, within the bound.
A program may use at most 128 MiB of HBM per device.

```python
import math
import jax
import jax.numpy as jnp
import numpy as np
from jax import lax

D = 2048
F = 1024
SCAN_CHANNELS = 1024
HW = 64
CONV_W = 4
TOP_K = 2
TOK_DEV = 160
EXPERTS = 8
STEP_COUNT = 1280
CAP = 80
N_SP = 8
N_TP = 4


DECAY_SCALE = 8.0


def decay_rates(key):
    base = jax.random.fold_in(key, 11)
    keys = jax.random.split(base, 3)
    share = 0.5
    fast = jax.random.uniform(keys[0], (2, SCAN_CHANNELS), jnp.float32) < share
    slow_rate = jnp.exp(jax.random.uniform(keys[1], (2, SCAN_CHANNELS), jnp.float32, math.log(0.005), math.log(0.05))) / STEP_COUNT
    fast_rate = jnp.exp(jax.random.uniform(keys[2], (2, SCAN_CHANNELS), jnp.float32, math.log(0.0025), math.log(0.008)))
    return jnp.where(fast, fast_rate, slow_rate)


def draw_decay_param(key, part):
    rate = decay_rates(key)
    return (-jnp.log(jnp.expm1(rate))).astype(jnp.float32)


def draw_decay_shift(key, part):
    rate = decay_rates(key)
    keys = jax.random.split(jax.random.fold_in(key, 12), 3)
    blocks = STEP_COUNT // TOK_DEV
    pace = jnp.exp(jax.random.uniform(keys[0], (2, blocks, SCAN_CHANNELS), jnp.float32, math.log(1.25), math.log(4.0)))
    pace_rows = jnp.repeat(pace, TOK_DEV, axis=1)
    filtered_signal = -DECAY_SCALE * 0.5 * rate[:, None, :] * (pace_rows - 1.0)
    expert_seats = jax.random.randint(keys[1], (2, 2, SCAN_CHANNELS), 0, STEP_COUNT)
    stack_level = jax.random.uniform(keys[2], (2, 2, SCAN_CHANNELS), jnp.float32, 0.2, 0.45)
    step_location = jnp.arange(STEP_COUNT, dtype=jnp.int32)[None, :, None]
    tally_clusters = jnp.zeros((2, STEP_COUNT, SCAN_CHANNELS), jnp.float32)
    for step_number in range(2):
        tally_clusters = tally_clusters + jnp.where(step_location == expert_seats[:, step_number][:, None, :], jnp.log1p(-stack_level[:, step_number])[:, None, :], 0.0)
    return (filtered_signal + tally_clusters).astype(jnp.float32)


def draw_saved_input(key, part):
    keys = jax.random.split(jax.random.fold_in(key, 13), 4)
    noise = jnp.clip(jax.random.normal(keys[0], (STEP_COUNT, D), jnp.float32), -4.0, 4.0)
    mixed = noise
    row_scale = jnp.exp(jax.random.uniform(keys[2], (STEP_COUNT, 1), jnp.float32, math.log(0.5), math.log(5.0)))
    column_scale = jnp.exp(jax.random.uniform(keys[3], (1, D), jnp.float32, math.log(0.3), math.log(3.0)))
    return (mixed * row_scale * column_scale).astype(jnp.bfloat16)


def with_spikes(values, rng, source, target, shards_of, factor):
    def block_of(dim):
        return (jnp.arange(values.shape[dim]) // (values.shape[dim] // shards_of)).reshape((-1,) + (1,) * (values.ndim - 1 - dim))

    near = jax.random.permutation(rng, shards_of)[block_of(target)]
    other_side = (block_of(target) + shards_of // 2) % shards_of
    return jnp.where((block_of(source) == near) | (block_of(source) == other_side), factor * values, values)


def block_scale(own_key, shape, cuts, least, largest):
    def one(axis_at, parts):
        draws = jax.random.uniform(jax.random.fold_in(jax.random.fold_in(own_key, 6), axis_at), (parts,), jnp.float32, least / len(cuts), largest / len(cuts))
        return jnp.repeat(jnp.exp(draws), shape[axis_at] // parts).reshape((-1,) + (1,) * (len(shape) - axis_at - 1))

    loudness = one(*cuts[0])
    for cut in cuts[1:]:
        loudness = loudness * one(*cut)
    return loudness


def shared_out(rng, own, number, rows, amount, top, most, lean):
    sequence = jax.random.permutation(rng, amount)
    crowded, ordinary = load_shares(amount, rows * top, most, lean, True), load_shares(amount, rows * top, most, lean, False)
    places = jnp.arange(amount)

    def named(lengths, rotation):
        used = int((lengths > 0).sum())
        fixed = max(1, used // 4)
        passed = fixed + (places - fixed + rotation * (used - fixed)) % max(1, amount - fixed)
        return jnp.zeros((amount,), jnp.int32).at[sequence[jnp.where(places < fixed, places, passed)]].set(jnp.asarray(lengths, jnp.int32))

    lengths = jnp.where(number % 4 == 0, named(crowded, number // 4), named(ordinary, number - number // 4 - 1))
    mixed = jax.random.permutation(jax.random.fold_in(own, 3), amount)
    source_of, receiver = mixed[0:amount // 2 * 2:2], mixed[1:amount // 2 * 2:2]
    margin = jnp.minimum(lengths[source_of] - 1, most - lengths[receiver]) // 2
    margin = jnp.where((source_of == sequence[0]) | (receiver == sequence[0]) | (lengths[receiver] == 0), 0, jnp.maximum(margin, 0))
    passed = jax.random.randint(jax.random.fold_in(own, 4), (amount // 2,), 0, 1 << 20) % (margin + 1)
    lengths = lengths.at[source_of].add(-passed).at[receiver].add(passed)
    items = jnp.searchsorted(jnp.cumsum(lengths), jnp.arange(rows * top), side="right").astype(jnp.int32)
    grid = items.reshape(top, rows).T
    grid = grid[jax.random.permutation(jax.random.fold_in(own, 1), rows)]
    rotation = jax.random.randint(jax.random.fold_in(own, 2), (rows, 1), 0, top)
    return jnp.take_along_axis(grid, (jnp.arange(top)[None, :] + rotation) % top, axis=1)


def load_shares(amount, total, bound, skew, full):
    loads = [(1 << 20) // math.isqrt(grade ** skew) + 1 for grade in range(1, amount + 1)]
    largest = bound if full else min(bound, max(-(-total // amount), total * loads[0] // sum(loads)))
    least = 1 if total - largest >= amount - 1 else 0
    given, spare = [largest] + [least] * (amount - 1), total - largest - least * (amount - 1)
    while spare > 0:
        free = [i for i in range(1, amount) if given[i] < largest] or [i for i in range(1, amount) if given[i] < bound]
        pool, left = sum([loads[i] for i in free]), spare
        for i in free:
            more = min(bound - given[i], max(1, left * loads[i] // pool), spare)
            given[i] = given[i] + more
            spare = spare - more
    return np.array(given)


def bell_draw(rng, shape, spread, reach, cuts=(), kind=jnp.bfloat16):
    result = spread * jax.random.normal(rng, shape, jnp.float32)
    if cuts:
        result = result * block_scale(rng, shape, cuts, -0.22, 0.18)
    return jnp.clip(result, -reach, reach).astype(kind)


def bell_draw_with(rng, shape, deviation, most, cuts, heavy, kind=jnp.bfloat16):
    result = deviation * jax.random.normal(rng, shape, jnp.float32)
    if cuts:
        result = result * block_scale(rng, shape, cuts, -0.22, 0.18)
    return jnp.clip(with_spikes(result, jax.random.fold_in(rng, 3), *heavy), -most, most).astype(kind)


def setup_inputs(seed: int = 0) -> dict:
    key_list = jax.random.split(jax.random.key(seed), 16)
    cotangent = bell_draw_with(key_list[0], (STEP_COUNT, D), 1.0, 8.0, ((0, 8),), (0, 1, 8, 2.0))
    saved_input = draw_saved_input(jax.random.fold_in(key_list[15], 71), 0)
    routes_keys = jax.random.split(jax.random.fold_in(key_list[2], 1), STEP_COUNT // TOK_DEV)
    routes_turns = jax.random.permutation(jax.random.fold_in(key_list[2], 3), STEP_COUNT // TOK_DEV)
    routes = jax.vmap(lambda own, number: shared_out(jax.random.fold_in(key_list[2], 2), own, number, TOK_DEV, EXPERTS, TOP_K, CAP, 1))(routes_keys, routes_turns).reshape((STEP_COUNT, TOP_K))
    route_weight = jnp.clip(0.2 + 1.3 * jax.random.uniform(key_list[3], (STEP_COUNT, TOP_K), jnp.float32) ** block_scale(key_list[3], (STEP_COUNT, TOP_K), ((0, 8),), -0.2, 0.2), 0.2, 1.5)
    gate_proj = bell_draw(key_list[4], (EXPERTS, D, F), D ** -0.5, 0.125, ((0, 8), (2, 4)))
    up_proj = bell_draw(key_list[5], (EXPERTS, D, F), D ** -0.5, 0.125, ((0, 8), (2, 4)))
    down_proj = bell_draw(key_list[6], (EXPERTS, F, D), F ** -0.5, 0.1875, ((0, 8), (1, 4)))
    out_proj = bell_draw(key_list[7], (D, SCAN_CHANNELS), SCAN_CHANNELS ** -0.5, 0.1875, ((1, 4),))
    conv_input = bell_draw(key_list[8], (STEP_COUNT, SCAN_CHANNELS), 1.0, 6.0, ((0, 8), (1, 4)))
    gate_branch = bell_draw(key_list[9], (STEP_COUNT, SCAN_CHANNELS), 1.0, 6.0, ((0, 8), (1, 4)))
    conv_taps = bell_draw(key_list[10], (CONV_W, SCAN_CHANNELS), 0.5, 3.0, ((1, 4),))
    recur_map = bell_draw(key_list[11], (2, SCAN_CHANNELS // HW, HW, HW), HW ** -0.5, 0.75, ((1, 4),))
    input_map = bell_draw(key_list[12], (2, SCAN_CHANNELS // HW, HW, HW), HW ** -0.5, 0.75, ((1, 4),))
    decay_param = draw_decay_param(jax.random.fold_in(key_list[15], 71), 0)
    decay_shift = draw_decay_shift(jax.random.fold_in(key_list[15], 71), 0)
    return {"cotangent": cotangent, "saved_input": saved_input, "routes": routes, "route_weight": route_weight, "gate_proj": gate_proj, "up_proj": up_proj, "down_proj": down_proj, "out_proj": out_proj, "conv_input": conv_input, "gate_branch": gate_branch, "conv_taps": conv_taps, "recur_map": recur_map, "input_map": input_map, "decay_param": decay_param, "decay_shift": decay_shift}


EPS = 1e-06
DECAY_SCALE = 8.0

def block_matrix(maps):
    heads = maps.shape[0]
    eye = jnp.eye(heads, dtype=jnp.float32)
    full = jnp.einsum('hij,hg->higj', maps.astype(jnp.float32), eye)
    return full.reshape(heads * maps.shape[1], heads * maps.shape[2])

def gate_terms(conv_out, recur_map, input_map, decay_param, decay_shift):
    recur = jax.nn.sigmoid(jnp.dot(conv_out, block_matrix(recur_map), precision=lax.Precision.HIGHEST))
    inputs = jax.nn.sigmoid(jnp.dot(conv_out, block_matrix(input_map), precision=lax.Precision.HIGHEST))
    log_decay = -DECAY_SCALE * recur * jax.nn.softplus(-decay_param)[None, :] + decay_shift
    decay = jnp.exp(log_decay)
    drive = jnp.sqrt(-jnp.expm1(2.0 * log_decay)) * (inputs * conv_out)
    return (decay, drive)

def link(earlier, later):
    return (earlier[0] * later[0], later[0] * earlier[1] + later[1])

def reference(cotangent, saved_input, routes, route_weight, gate_proj, up_proj, down_proj, out_proj, conv_input, gate_branch, conv_taps, recur_map, input_map, decay_param, decay_shift):
    inputs32 = saved_input.astype(jnp.float32)
    inv_rms = lax.rsqrt(lax.optimization_barrier(jnp.mean(inputs32 * inputs32, axis=1, keepdims=True)) + EPS)
    normed = inputs32 * inv_rms
    expert_input = normed.astype(jnp.bfloat16)
    scaled = (route_weight[:, :, None] * cotangent.astype(jnp.float32)[:, None, :]).astype(jnp.bfloat16)
    scaled = scaled.reshape(STEP_COUNT * TOP_K, D)
    flat_expert = routes.reshape(-1).astype(jnp.int32)
    order = jnp.argsort(flat_expert, stable=True).astype(jnp.int32)
    counts = lax.optimization_barrier(jnp.sum((flat_expert[:, None] == jnp.arange(EXPERTS, dtype=jnp.int32)[None, :]).astype(jnp.int32), axis=0)).astype(jnp.int32)
    starts = (jnp.cumsum(counts) - counts).astype(jnp.int32)
    most_rows = N_SP * CAP
    padded_order = jnp.concatenate([order, jnp.zeros((most_rows,), jnp.int32)])
    block = F // N_TP

    def one_expert(expert):
        picks = lax.dynamic_slice_in_dim(padded_order, starts[expert], most_rows)
        live = jnp.arange(most_rows, dtype=jnp.int32) < counts[expert]
        rows_input = jnp.where(live[:, None], expert_input[picks // TOP_K], 0.0).astype(jnp.bfloat16)
        rows_scaled = jnp.where(live[:, None], scaled[picks], 0.0).astype(jnp.bfloat16)
        w_gate = gate_proj[expert]
        w_up = up_proj[expert]
        w_down = down_proj[expert]
        gate_pre = jnp.dot(rows_input, w_gate, preferred_element_type=jnp.float32)
        up_pre = jnp.dot(rows_input, w_up, preferred_element_type=jnp.float32)
        gate_sig = jax.nn.sigmoid(gate_pre)
        gate_act = gate_pre * gate_sig
        hidden = (gate_act * up_pre).astype(jnp.bfloat16)
        hidden_grad = jnp.dot(rows_scaled, w_down.T, preferred_element_type=jnp.float32)
        gate_grad = (hidden_grad * up_pre * gate_sig * (1.0 + gate_pre * (1.0 - gate_sig))).astype(jnp.bfloat16)
        up_grad = (hidden_grad * gate_act).astype(jnp.bfloat16)
        grad_down = jnp.dot(hidden.T, rows_scaled, preferred_element_type=jnp.float32)
        grad_gate = jnp.dot(rows_input.T, gate_grad, preferred_element_type=jnp.float32)
        grad_up = jnp.dot(rows_input.T, up_grad, preferred_element_type=jnp.float32)
        pieces = jnp.zeros((most_rows, D), jnp.float32)
        for step_number in range(N_TP):
            low = step_number * block
            piece = jnp.dot(gate_grad[:, low:low + block], w_gate[:, low:low + block].T, preferred_element_type=jnp.float32)
            piece = piece + jnp.dot(up_grad[:, low:low + block], w_up[:, low:low + block].T, preferred_element_type=jnp.float32)
            rounded = lax.optimization_barrier(piece.astype(jnp.bfloat16))
            pieces = pieces + rounded.astype(jnp.float32)
        route_rows = pieces.astype(jnp.bfloat16)
        target = jnp.where(live, picks, STEP_COUNT * TOP_K).astype(jnp.int32)
        return (grad_gate, grad_up, grad_down, route_rows, target)
    grad_gate_proj, grad_up_proj, grad_down_proj, route_rows, targets = lax.map(one_expert, jnp.arange(EXPERTS, dtype=jnp.int32))
    assigned = jnp.zeros((STEP_COUNT * TOP_K + 1, D), jnp.bfloat16).at[targets.reshape(-1)].set(route_rows.reshape(-1, D))
    normed_grad = lax.optimization_barrier(jnp.sum(assigned[:STEP_COUNT * TOP_K].reshape(STEP_COUNT, TOP_K, D).astype(jnp.float32), axis=1))
    mixed_grad = cotangent.astype(jnp.float32) + inv_rms * (normed_grad - normed * lax.optimization_barrier(jnp.mean(normed_grad * normed, axis=1, keepdims=True)))
    mixed_grad_b = mixed_grad.astype(jnp.bfloat16)
    taps32 = conv_taps.astype(jnp.float32)

    def mixer(conv_in, branch):
        padded = jnp.pad(conv_in, ((2, 1), (0, 0)))
        conv_out = jnp.zeros((STEP_COUNT, SCAN_CHANNELS), jnp.float32)
        for offset in range(CONV_W):
            conv_out = conv_out + padded[offset:offset + STEP_COUNT] * taps32[offset]
        states = jnp.zeros((STEP_COUNT, SCAN_CHANNELS), jnp.float32)
        for direction in range(2):
            decay, drive = gate_terms(conv_out, recur_map[direction], input_map[direction], decay_param[direction], decay_shift[direction])
            states = states + lax.associative_scan(link, (decay, drive), axis=0, reverse=direction == 1)[1]
        return jax.nn.gelu(branch) * states
    value, pull = jax.vjp(mixer, conv_input.astype(jnp.float32), gate_branch.astype(jnp.float32))
    mixed_out = value.astype(jnp.bfloat16)
    grad_out_proj = lax.dot_general(mixed_grad_b, mixed_out, (((0,), (0,)), ((), ())), preferred_element_type=jnp.float32)
    out_grad = jnp.dot(mixed_grad_b, out_proj, preferred_element_type=jnp.float32)
    conv_grad, branch_grad = pull(out_grad)
    return (grad_gate_proj, grad_up_proj, grad_down_proj, grad_out_proj, conv_grad.astype(jnp.bfloat16), branch_grad.astype(jnp.bfloat16))
```

```python
import functools
import jax
import jax.numpy as jnp
from jax import lax
from jax.experimental import pallas as pl
from jax.experimental.pallas import tpu as pltpu
from jax.sharding import PartitionSpec as P

EPS = 1e-06
DECAY_SCALE = 8.0
ROW_TILE = 16
GROUPS = 4
LAG = 2
GELU_K = 0.7978845608028654
GELU_C = 0.044715
VM = pl.BlockSpec(memory_space=pltpu.VMEM)
HB = pl.BlockSpec(memory_space=pltpu.HBM)
BF = jnp.bfloat16
F32 = jnp.float32
ROWS0 = (((0,), (0,)), ((), ()))
COLS1 = (((1,), (1,)), ((), ()))
PLAIN = (((1,), (0,)), ((), ()))


def neighbours():
    tp = lax.axis_index("tp")
    side = tp // 2
    core = tp % 2
    return tp, side * 2 + (1 - core), (1 - side) * 2 + core, (1 - side) * 2 + (1 - core)


def partner_at(sp, n, d):
    if n & (n - 1):
        return (sp + d) % n
    bit, peer = 1, sp
    while bit < n:
        if d & bit:
            peer = peer + bit * (1 - 2 * ((sp // bit) % 2))
        bit *= 2
    return peer


def source_at(sp, n, d):
    return (sp + n - d) % n if n & (n - 1) else partner_at(sp, n, d)


def announce(n, tps):
    sp = lax.axis_index("sp")
    tp = lax.axis_index("tp")
    barrier = pltpu.get_barrier_semaphore()
    for d in range(1, n):
        pl.semaphore_signal(
            barrier, inc=1, device_id=((sp + d) % n, tp), device_id_type=pl.DeviceIdType.MESH
        )
    for other in tps:
        pl.semaphore_signal(barrier, inc=1, device_id=(sp, other), device_id_type=pl.DeviceIdType.MESH)
    return barrier, n - 1 + len(tps)


def remote(src, dst, sems, index, device):
    return pltpu.make_async_remote_copy(
        src_ref=src,
        dst_ref=dst,
        send_sem=sems.at[(0,) + index],
        recv_sem=sems.at[(1,) + index],
        device_id=device,
        device_id_type=pl.DeviceIdType.MESH,
    )


def edge_copies(n, x_ref, halo_ref, sems):
    sp = lax.axis_index("sp")
    tp = lax.axis_index("tp")
    length, tile = x_ref.shape[0], halo_ref.shape[1]
    copies = (
        remote(x_ref.at[pl.ds(length - tile, tile)], halo_ref.at[0], sems, (0,), ((sp + 1) % n, tp)),
        remote(x_ref.at[pl.ds(0, tile)], halo_ref.at[1], sems, (1,), ((sp + n - 1) % n, tp)),
    )
    for copy in copies:
        copy.start()
    return copies


def halo_rows(halo_ref, n):
    sp = lax.axis_index("sp")
    before = jnp.where(sp == 0, 0.0, halo_ref[0].astype(F32))
    after = jnp.where(sp == n - 1, 0.0, halo_ref[1].astype(F32))
    return before[before.shape[0] - 2 :], after[:2]


def split_dot(x, w, dims):
    high = x.astype(BF)
    low = (x - high.astype(F32)).astype(BF)
    total = lax.dot_general(low, w, dims, preferred_element_type=F32)
    return total + lax.dot_general(high, w, dims, preferred_element_type=F32)


def minus_expm1(y):
    series = 1.0 + y * (1.0 / 8.0)
    for k in (7.0, 6.0, 5.0, 4.0, 3.0, 2.0):
        series = 1.0 + y * (1.0 / k) * series
    return jnp.where(y > -0.25, -y * series, 1.0 - jnp.exp(y))


def shifted(x, by, edge):
    length = x.shape[0]
    row = lax.broadcasted_iota(jnp.int32, x.shape, 0)
    moved = pltpu.roll(x, by % length, 0)
    return jnp.where(row == (0 if by > 0 else length - 1), edge, moved)


def run_scans(length, jobs):
    width = jobs[0][1].shape[1]
    groups = length // 8

    def body(g, carry):
        out = []
        for (reverse, a_ref, b_ref, to_ref), state in zip(jobs, carry):
            base = pl.multiple_of((groups - 1 - g if reverse else g) * 8, 8)
            a = a_ref[pl.ds(base, 8), :]
            b = None if b_ref is None else b_ref[pl.ds(base, 8), :]
            rows = [None] * 8
            for k in reversed(range(8)) if reverse else range(8):
                state = a[k : k + 1] * state
                if b is not None:
                    state = state + b[k : k + 1]
                rows[k] = state
            to_ref[pl.ds(base, 8), :] = jnp.concatenate(rows, axis=0)
            out.append(state)
        return tuple(out)

    start = tuple(
        jnp.full((1, width), 1.0 if b_ref is None else 0.0, F32) for _, _, b_ref, _ in jobs
    )
    return lax.fori_loop(0, groups, body, start)


def gelu_parts(x):
    t = jnp.tanh(GELU_K * (x + GELU_C * x * x * x))
    value = 0.5 * x * (1.0 + t)
    slope = 0.5 * (1.0 + t) + 0.5 * x * (1.0 - t * t) * GELU_K * (1.0 + 3.0 * GELU_C * x * x)
    return value, slope


def carries(n, all_ref, rows):
    sp = lax.axis_index("sp")
    zero = jnp.zeros((1, all_ref.shape[2]), F32)
    (lp, le), (up, ue) = rows

    def lower(k, carry):
        t = all_ref[k]
        return t[lp : lp + 1] * carry + t[le : le + 1]

    def upper(i, carry):
        t = all_ref[n - 1 - i]
        return t[up : up + 1] * carry + t[ue : ue + 1]

    return lax.fori_loop(0, sp, lower, zero), lax.fori_loop(0, n - 1 - sp, upper, zero)


def front_kernel(n, slots, *refs):
    (
        cot_hbm, x_hbm, routes_ref, weight_ref, wg_hbm, wu_hbm, wd_hbm, cin_ref, branch_ref,
        taps_ref, rmap_ref, imap_ref, plus_ref, shift_hbm,
        ng_ref, ggate_ref, gup_ref, gdown_ref,
        maps_ref, decay_ref, ones_ref, a_ref, c_ref, e_ref, value_ref, slope_ref, mixed_out_ref,
        tot_ref,
        cot_ref, x_ref, nx_ref, wg_ref, wu_ref, wd_ref, shift_ref,
        rank_ref, pick_ref, send_ref, wide_ref, rows_sc, rows_in, hid_ref, ggu_ref, part_ref,
        got1, got2, mid, fin, back, halo_ref,
        conv_ref, gates_ref, root_ref, drive_ref, state_ref, cum_ref, all_ref,
        loc, edge, hop, wide, pair, cross, fwd, s_pair, s_cross, s_hop, s_tail, s_tot,
    ) = refs
    length, width = cot_ref.shape
    fourth = send_ref.shape[3]
    channels = cin_ref.shape[1]
    sp = lax.axis_index("sp")
    tp, partner, across, diagonal = neighbours()
    per = n // GROUPS
    rows = (rows_sc, rows_in)

    def cols(q):
        return pl.ds(pl.multiple_of(q * fourth, 128), fourth)

    barrier, heard = announce(n, (partner, across))
    loads = [
        pltpu.make_async_copy(src, dst, loc.at[i])
        for i, (src, dst) in enumerate(
            (
                (x_hbm, x_ref), (cot_hbm, cot_ref), (shift_hbm, shift_ref),
                (wg_hbm, wg_ref), (wu_hbm, wu_ref), (wd_hbm, wd_ref),
            )
        )
    ]
    for load in loads:
        load.start()

    route0, route1 = routes_ref[0:1], routes_ref[1:2]
    which = lax.broadcasted_iota(jnp.int32, (n, length), 0)
    named = ((which == route0) | (which == route1)).astype(F32).astype(BF)
    earlier = lax.broadcasted_iota(jnp.int32, (length, length), 0) < lax.broadcasted_iota(
        jnp.int32, (length, length), 1
    )
    rank_ref[...] = jnp.dot(named, earlier.astype(F32).astype(BF), preferred_element_type=F32)
    loads[0].wait()
    for r in range(0, length, 32):
        x = x_ref[r : r + 32].astype(F32)
        inv = lax.rsqrt(jnp.mean(x * x, axis=1, keepdims=True) + EPS)
        nx_ref[r : r + 32] = (x * inv).astype(BF)
    loads[1].wait()

    def chosen(d):
        e = partner_at(sp, n, d)
        rank = rank_ref[pl.ds(e, 1), :].astype(jnp.int32)
        slot = lax.broadcasted_iota(jnp.int32, (slots, length), 0) == rank
        hit0 = slot & (route0 == e)
        hit1 = slot & (route1 == e)
        pick = (hit0 | hit1).astype(F32).astype(BF)
        pick_ref[d * slots : (d + 1) * slots] = pick
        share = jnp.where(hit0, weight_ref[0:1], 0.0) + jnp.where(hit1, weight_ref[1:2], 0.0)
        return pick, jnp.sum(share, axis=1, keepdims=True)

    def taken(pick, share, where):
        got = jnp.dot(pick, nx_ref[:, where], preferred_element_type=F32).astype(BF)
        cot = jnp.dot(pick, cot_ref[:, where], preferred_element_type=F32)
        return (cot * share).astype(BF), got

    near_d = [d for d in (1,) if d < n]
    far = [d for d in range(2, n)]
    order = near_d + [d for g in range(GROUPS - 1, -1, -1) for d in far if d // per == g]
    hops, extra, pending = {}, {}, []
    pl.semaphore_wait(barrier, heard)
    edges = edge_copies(n, cin_ref, halo_ref, edge)
    for d in order:
        peer = partner_at(sp, n, d)
        pick, share = chosen(d)
        for a, value in enumerate(taken(pick, share, cols(tp))):
            send_ref[a, d] = value
            copy = remote(send_ref.at[a, d], rows[a].at[d, :, cols(tp)], hop, (a, d), (peer, tp))
            copy.start()
            hops[a, d] = copy
        if d in near_d:
            for a, value in enumerate(taken(pick, share, cols(across))):
                i = near_d.index(d)
                wide_ref[a, i] = value
                copy = remote(
                    wide_ref.at[a, i], rows[a].at[d, :, cols(across)], wide, (a, i), (peer, tp)
                )
                copy.start()
                extra[a, d] = copy
    pick, share = chosen(0)
    for q in range(width // fourth):
        where = pl.ds(q * fourth, fourth)
        rows_sc[0, :, where], rows_in[0, :, where] = taken(pick, share, where)

    heads, hw = rmap_ref.shape[1], rmap_ref.shape[2]
    spread = (
        lax.broadcasted_iota(jnp.int32, (hw, channels), 1) % hw
        == lax.broadcasted_iota(jnp.int32, (hw, channels), 0)
    ).astype(F32).astype(BF)
    block = (
        lax.broadcasted_iota(jnp.int32, (channels, channels), 0) // hw
        == lax.broadcasted_iota(jnp.int32, (channels, channels), 1) // hw
    )
    for i in range(4):
        stack = (rmap_ref, imap_ref)[i % 2][i // 2].reshape(heads * hw, hw)
        full = jnp.dot(stack, spread, preferred_element_type=F32)
        maps_ref[:, i * channels : (i + 1) * channels] = jnp.where(block, full, 0.0).astype(BF)
    for copy in edges:
        copy.wait()
    taps = taps_ref[...].astype(F32)
    low, high = halo_rows(halo_ref, n)
    x = cin_ref[...].astype(F32)
    back1 = shifted(x, 1, low[1:2])
    back2 = shifted(back1, 1, low[0:1])
    conv = back2 * taps[0:1] + back1 * taps[1:2] + x * taps[2:3]
    conv = conv + shifted(x, -1, high[0:1]) * taps[3:4]
    conv_ref[...] = conv
    gates_ref[...] = jax.nn.sigmoid(split_dot(conv, maps_ref[...], PLAIN))
    loads[2].wait()
    for d in range(2):
        recur = gates_ref[:, 2 * d * channels : (2 * d + 1) * channels]
        inputs = gates_ref[:, (2 * d + 1) * channels : (2 * d + 2) * channels]
        log_decay = -DECAY_SCALE * recur * plus_ref[d : d + 1, :] + shift_ref[d]
        root = jnp.sqrt(minus_expm1(2.0 * log_decay))
        decay_ref[d] = jnp.exp(log_decay)
        root_ref[d] = root
        drive_ref[d] = root * (inputs * conv_ref[...])
    a_f, a_b = decay_ref.at[0], decay_ref.at[1]
    ends = run_scans(
        length,
        (
            (False, a_f, drive_ref.at[0], state_ref.at[0]),
            (True, a_b, drive_ref.at[1], state_ref.at[1]),
            (False, a_f, None, cum_ref.at[0]),
            (True, a_b, None, cum_ref.at[1]),
            (True, a_f, None, ones_ref.at[0]),
            (False, a_b, None, ones_ref.at[1]),
        ),
    )
    tot_ref[0:1, :] = ends[2]
    tot_ref[1:2, :] = ends[0]
    tot_ref[2:3, :] = ends[3]
    tot_ref[3:4, :] = ends[1]
    tot_ref[4:8, :] = jnp.zeros((4, channels), F32)
    totals = []
    for d in range(n - 1, 0, -1):
        copy = remote(tot_ref, all_ref.at[sp], s_tot, (d,), (partner_at(sp, n, d), tp))
        copy.start()
        totals.append(copy)
    all_ref[sp] = tot_ref[...]

    def finish_states():
        for copy in totals:
            copy.wait()
        in_f, in_b = carries(n, all_ref, ((0, 1), (2, 3)))
        state_f = state_ref[0] + cum_ref[0] * in_f
        state_b = state_ref[1] + cum_ref[1] * in_b
        beside = (shifted(state_f, 1, in_f), shifted(state_b, -1, in_b))
        value, slope = gelu_parts(branch_ref[...].astype(F32))
        states = state_f + state_b
        value_ref[...] = value
        slope_ref[...] = states * slope
        mixed_out_ref[...] = (value * states).astype(BF)
        conv = conv_ref[...]
        for d in range(2):
            recur = gates_ref[:, 2 * d * channels : (2 * d + 1) * channels]
            inputs = gates_ref[:, (2 * d + 1) * channels : (2 * d + 2) * channels]
            decay = decay_ref[d]
            root = root_ref[d]
            a_ref[d] = root * inputs
            g_log = beside[d] * decay - inputs * conv * (decay * decay) / root
            c_ref[d] = g_log * (-DECAY_SCALE * plus_ref[d : d + 1, :]) * recur * (1.0 - recur)
            e_ref[d] = root * conv * inputs * (1.0 - inputs)

    nears, fwds, overs, late = {}, {}, {}, []

    def step_in(a, d):
        hops[a, d].wait_recv()
        dst = rows[a]
        mine = dst.at[d, :, cols(tp)]
        if d in near_d:
            extra[a, d].wait_recv()
            other = dst.at[d, :, cols(across)]
            fwds[a, d] = remote(other, other, fwd, (a, d), (sp, partner))
            fwds[a, d].start()
        else:
            overs[a, d] = remote(mine, mine, cross, (a, d), (sp, across))
            overs[a, d].start()
            late.append((a, d))
        nears[a, d] = remote(mine, mine, pair, (a, d), (sp, partner))
        nears[a, d].start()

    def step_on():
        a, d = late.pop(0)
        overs[a, d].wait_recv()
        other = rows[a].at[d, :, cols(across)]
        fwds[a, d] = remote(other, other, fwd, (a, d), (sp, partner))
        fwds[a, d].start()

    def bring(g):
        for d in order:
            if d // per == g:
                for a in range(2):
                    step_in(a, d)
                    if len(late) > LAG:
                        step_on()

    pairs, crosses, backs = {}, {}, {}

    def experts(g):
        while any(d // per == g for _, d in late):
            step_on()
        for d in range(g * per, (g + 1) * per):
            if d:
                for a in range(2):
                    nears[a, d].wait_recv()
                    fwds[a, d].wait_recv()
        count = per * slots
        at = slice(g * count, (g + 1) * count)
        xin = rows_in[g * per : (g + 1) * per].reshape(count, width)
        gate_pre = jnp.dot(xin, wg_ref[...], preferred_element_type=F32)
        up_pre = jnp.dot(xin, wu_ref[...], preferred_element_type=F32)
        xsc = rows_sc[g * per : (g + 1) * per].reshape(count, width)
        hidden_grad = lax.dot_general(xsc, wd_ref[...], COLS1, preferred_element_type=F32)
        gate_sig = jax.nn.sigmoid(gate_pre)
        gate_act = gate_pre * gate_sig
        hid_ref[at] = (gate_act * up_pre).astype(BF)
        gate_grad = hidden_grad * up_pre * gate_sig * (1.0 + gate_pre * (1.0 - gate_sig))
        gate_grad = gate_grad.astype(BF)
        up_grad = (hidden_grad * gate_act).astype(BF)
        units = up_grad.shape[1]
        ggu_ref[at, :units] = gate_grad
        ggu_ref[at, units:] = up_grad
        for i, q in enumerate((diagonal, partner, across, tp)):
            some = pl.ds(pl.multiple_of(q * fourth, 128), fourth)
            total = lax.dot_general(gate_grad, wg_ref[some], COLS1, preferred_element_type=F32)
            total = total + lax.dot_general(up_grad, wu_ref[some], COLS1, preferred_element_type=F32)
            part_ref[g * per : (g + 1) * per, :, cols(q)] = total.astype(BF).reshape(
                per, slots, fourth
            )
            if i < 2:
                for d in range(g * per, (g + 1) * per):
                    copy = remote(
                        part_ref.at[d, :, cols(q)], got1.at[i, d], s_pair, (i, d), (sp, partner)
                    )
                    copy.start()
                    pairs[i, d] = copy

    def stage_b(g):
        for d in range(g * per, (g + 1) * per):
            pairs[0, d].wait_recv()
            total = part_ref[d, :, cols(across)].astype(F32) + got1[0, d].astype(F32)
            mid[d] = total.astype(BF)
            crosses[d] = remote(mid.at[d], got2.at[d], s_cross, (d,), (sp, across))
            crosses[d].start()

    def stage_c(g):
        for d in range(g * per, (g + 1) * per):
            pairs[1, d].wait_recv()
            crosses[d].wait_recv()
            total = part_ref[d, :, cols(tp)].astype(F32) + got1[1, d].astype(F32)
            total = (total + got2[d].astype(F32)).astype(BF)
            if d == 0:
                back[0] = total
            else:
                fin[d] = total
                backs[d] = remote(fin.at[d], back.at[d], s_hop, (d,), (source_at(sp, n, d), tp))
                backs[d].start()

    chunk = width // 8

    def weight_gradients(k):
        at = slice(k * chunk, (k + 1) * chunk)
        units = hid_ref.shape[1]
        left = rows_in[:, :, at].reshape(n * slots, chunk)
        both = lax.dot_general(left, ggu_ref[...], ROWS0, preferred_element_type=F32)
        ggate_ref[at] = both[:, :units]
        gup_ref[at] = both[:, units:]
        right = rows_sc[:, :, at].reshape(n * slots, chunk)
        gdown_ref[:, at] = lax.dot_general(hid_ref[...], right, ROWS0, preferred_element_type=F32)

    bring(0)
    bring(3)
    for i in (3, 4, 5):
        loads[i].wait()
    experts(0)
    bring(2)
    experts(3)
    stage_b(0)
    bring(1)
    experts(2)
    stage_b(3)
    stage_c(0)
    experts(1)
    stage_b(2)
    stage_c(3)
    stage_b(1)
    weight_gradients(0)
    weight_gradients(1)
    stage_c(2)
    weight_gradients(2)
    weight_gradients(3)
    stage_c(1)
    finish_states()
    for k in range(4, 8):
        weight_gradients(k)
    for d in range(1, n):
        backs[d].wait_recv()
    got = back[...].reshape(n * slots, fourth)
    grad = lax.dot_general(pick_ref[...], got, ROWS0, preferred_element_type=F32)
    ng_ref[:, cols(tp)] = grad.astype(BF)
    own = ng_ref.at[:, cols(tp)]
    over = remote(own, own, s_tail, (0,), (sp, across))
    near = remote(own, own, s_tail, (1,), (sp, partner))
    over.start()
    near.start()
    over.wait_recv()
    other = ng_ref.at[:, cols(across)]
    last = remote(other, other, s_tail, (2,), (sp, partner))
    last.start()
    for group in (hops, extra, nears, fwds, overs, pairs, crosses, backs):
        for copy in group.values():
            copy.wait_send()
    near.wait()
    over.wait_send()
    last.wait()


def front(args, plus, shapes, n, n_tp, slots):
    cot, x, routes, weight, wg, wu, wd, cin, branch, taps, rmap, imap, shift = args
    length, width = cot.shape
    channels = cin.shape[1]
    units = wg.shape[1]
    fourth = width // n_tp
    dma = pltpu.SemaphoreType.DMA
    sds = jax.ShapeDtypeStruct
    vm = pltpu.VMEM
    one, two = (length, channels), (2, length, channels)
    outs = (
        sds((length, width), BF),
        sds((width, units), F32),
        sds((width, units), F32),
        sds((units, width), F32),
        sds((channels, 4 * channels), BF),
        sds(two, F32), sds(two, F32), sds(two, F32), sds(two, F32), sds(two, F32),
        sds(one, F32), sds(one, F32), sds(one, BF),
        sds((8, channels), F32),
    )
    block = (n, slots, fourth)
    scratch = [
        vm((length, width), BF), vm((length, width), BF), vm((length, width), BF),
        vm((width, units), BF), vm((width, units), BF), vm((units, width), BF), vm(two, F32),
        vm((n, length), F32), vm((n * slots, length), BF), vm((2,) + block, BF),
        vm((2, 1, slots, fourth), BF),
        vm((n, slots, width), BF), vm((n, slots, width), BF),
        vm((n * slots, units), BF), vm((n * slots, 2 * units), BF), vm((n, slots, width), BF),
        vm((2,) + block, BF), vm(block, BF), vm(block, BF), vm(block, BF), vm(block, BF),
        vm((2, ROW_TILE, channels), BF),
        vm(one, F32), vm((length, 4 * channels), F32), vm(two, F32), vm(two, F32), vm(two, F32),
        vm(two, F32), vm((n, 8, channels), F32),
        dma((6,)), dma((2, 2)), dma((2, 2, n)), dma((2, 2, 1)), dma((2, 2, n)), dma((2, 2, n)),
        dma((2, 2, n)), dma((2, 2, n)), dma((2, n)), dma((2, n)), dma((2, 3)), dma((2, n)),
    ]
    return pl.pallas_call(
        functools.partial(front_kernel, n, slots),
        out_shape=outs,
        in_specs=[HB, HB, VM, VM, HB, HB, HB, VM, VM, VM, VM, VM, VM, HB],
        out_specs=[VM] * len(outs),
        scratch_shapes=scratch,
        compiler_params=pltpu.CompilerParams(
            collective_id=1, has_side_effects=True, vmem_limit_bytes=40 * 2**20
        ),
        cost_estimate=pl.CostEstimate(
            flops=2_000_000_000, bytes_accessed=30_000_000, transcendentals=0
        ),
    )(cot, x, routes, weight, wg, wu, wd, cin, branch, taps, rmap, imap, plus, shift)


def tail_kernel(n, *refs):
    (
        ng_ref, cot_ref, x_ref, proj_ref, decay_ref, ones_ref, a_ref, c_ref, e_ref, value_ref,
        slope_ref, maps_ref, tot_ref, mixed_out_ref, taps_ref,
        grad_out_ref, input_grad_ref, branch_grad_ref,
        mixed_ref, mixed_all, out_all, drive_ref, after_ref, msg_ref, all_ref, packed_ref,
        conv_grad_ref, halo_ref,
        s_tot, s_mix, s_pair, s_out, s_edge,
    ) = refs
    length, width = ng_ref.shape
    channels = decay_ref.shape[2]
    part = width // n
    half = length // 2
    sp = lax.axis_index("sp")
    tp, partner, _, _ = neighbours()
    barrier, heard = announce(n, (partner,))
    powers = n & (n - 1) == 0
    mine = pl.ds(pl.multiple_of((tp % 2) * half, ROW_TILE), half)

    out_all[0] = mixed_out_ref[...]
    pl.semaphore_wait(barrier, heard)
    gathers = []

    def gather(bit):
        got = []
        for d in range(0, n, 2 * bit):
            copy = remote(out_all.at[d], out_all.at[d + bit], s_out, (d + bit,), (partner_at(sp, n, bit), tp))
            copy.start()
            got.append(copy)
        gathers.append(got)

    bits = []
    if powers:
        bit = n // 2
        while bit:
            bits.append(bit)
            bit //= 2
        gather(bits.pop(0))
    else:
        got = []
        for d in range(1, n):
            copy = remote(out_all.at[0], out_all.at[d], s_out, (d,), (partner_at(sp, n, d), tp))
            copy.start()
            got.append(copy)
        gathers.append(got)

    def gather_on():
        if bits:
            for copy in gathers[-1]:
                copy.wait_recv()
            gather(bits.pop(0))

    for r in range(0, length, 32):
        x = x_ref[r : r + 32].astype(F32)
        inv = lax.rsqrt(jnp.mean(x * x, axis=1, keepdims=True) + EPS)
        normed = x * inv
        ng = ng_ref[r : r + 32].astype(F32)
        dot = jnp.mean(ng * normed, axis=1, keepdims=True)
        mixed = (cot_ref[r : r + 32].astype(F32) + inv * (ng - normed * dot)).astype(BF)
        for e in range(n):
            mixed_ref[e, r : r + 32] = mixed[:, e * part : (e + 1) * part]
    out_grad = jnp.zeros((length, channels), F32)
    for e in range(n):
        out_grad = out_grad + jnp.dot(
            mixed_ref[e], proj_ref[e * part : (e + 1) * part], preferred_element_type=F32
        )
    carried = out_grad * value_ref[...]
    branch_grad_ref[...] = (out_grad * slope_ref[...]).astype(BF)
    drive_ref[...] = decay_ref[...] * carried[None]
    ends = run_scans(
        length,
        (
            (True, decay_ref.at[0], drive_ref.at[0], after_ref.at[0]),
            (False, decay_ref.at[1], drive_ref.at[1], after_ref.at[1]),
        ),
    )
    msg_ref[0:1, :] = tot_ref[0:1, :]
    msg_ref[1:2, :] = tot_ref[2:3, :]
    msg_ref[2:3, :] = ends[1]
    msg_ref[3:4, :] = ends[0]
    msg_ref[4:8, :] = jnp.zeros((4, channels), F32)
    totals = []
    for d in range(n - 1, 0, -1):
        copy = remote(msg_ref, all_ref.at[sp], s_tot, (d,), (partner_at(sp, n, d), tp))
        copy.start()
        totals.append(copy)
    all_ref[sp] = msg_ref[...]
    mixes, pairs = {}, {}
    for d in range(n - 1, 0, -1):
        peer = partner_at(sp, n, d)
        mixes[d] = remote(mixed_ref.at[peer, mine], mixed_all.at[d, mine], s_mix, (d,), (peer, tp))
        mixes[d].start()
    mixed_all[0] = mixed_ref[sp]
    gather_on()
    for copy in totals:
        copy.wait()
    in_ab, in_af = carries(n, all_ref, ((1, 2), (0, 3)))
    after_f = after_ref[0] + ones_ref[0] * in_af
    after_b = after_ref[1] + ones_ref[1] * in_ab
    adjoint = (carried + shifted(after_f, -1, in_af), carried + shifted(after_b, 1, in_ab))
    total = adjoint[0] * a_ref[0] + adjoint[1] * a_ref[1]
    for d in range(2):
        packed_ref[:, 2 * d * channels : (2 * d + 1) * channels] = adjoint[d] * c_ref[d]
        packed_ref[:, (2 * d + 1) * channels : (2 * d + 2) * channels] = adjoint[d] * e_ref[d]
    total = total + split_dot(packed_ref[...], maps_ref[...], COLS1)
    conv_grad_ref[...] = total.astype(BF)
    edges = edge_copies(n, conv_grad_ref, halo_ref, s_edge)
    while bits:
        gather_on()
    for d in range(n - 1, 0, -1):
        mixes[d].wait_recv()
        block = mixed_all.at[d, mine]
        pairs[d] = remote(block, block, s_pair, (d,), (sp, partner))
        pairs[d].start()
    for copy in edges:
        copy.wait()
    taps = taps_ref[...].astype(F32)
    low, high = halo_rows(halo_ref, n)
    up1 = shifted(total, -1, high[0:1])
    up2 = shifted(up1, -1, high[1:2])
    down = shifted(total, 1, low[1:2])
    result = up2 * taps[0:1] + up1 * taps[1:2] + total * taps[2:3] + down * taps[3:4]
    input_grad_ref[...] = result.astype(BF)
    for d in range(1, n):
        pairs[d].wait()
        mixes[d].wait_send()
    for got in gathers[:-1]:
        for copy in got:
            copy.wait_send()
    for copy in gathers[-1]:
        copy.wait()
    grad_out_ref[...] = lax.dot_general(
        mixed_all[...].reshape(n * length, part),
        out_all[...].reshape(n * length, channels),
        ROWS0,
        preferred_element_type=F32,
    )


def tail(args, n):
    ng, proj, decay = args[0], args[3], args[4]
    length, width = ng.shape
    channels = proj.shape[1]
    part = width // n
    dma = pltpu.SemaphoreType.DMA
    sds = jax.ShapeDtypeStruct
    vm = pltpu.VMEM
    two = (2, length, channels)
    return pl.pallas_call(
        functools.partial(tail_kernel, n),
        out_shape=(
            sds((part, channels), F32), sds((length, channels), BF), sds((length, channels), BF),
        ),
        in_specs=[VM] * len(args),
        out_specs=[VM] * 3,
        scratch_shapes=[
            vm((n, length, part), BF), vm((n, length, part), BF), vm((n, length, channels), BF),
            vm(two, F32), vm(two, F32), vm((8, channels), F32), vm((n, 8, channels), F32),
            vm((length, 4 * channels), F32), vm((length, channels), BF),
            vm((2, ROW_TILE, channels), BF),
            dma((2, n)), dma((2, n)), dma((2, n)), dma((2, n)), dma((2, 2)),
        ],
        compiler_params=pltpu.CompilerParams(
            collective_id=2, has_side_effects=True, vmem_limit_bytes=24 * 2**20
        ),
        cost_estimate=pl.CostEstimate(
            flops=500_000_000, bytes_accessed=10_000_000, transcendentals=0
        ),
    )(*args)


def shards(
    cotangent,
    saved_input,
    routes,
    route_weight,
    gate_proj,
    up_proj,
    down_proj,
    out_proj,
    conv_input,
    gate_branch,
    conv_taps,
    recur_map,
    input_map,
    decay_param,
    decay_shift,
):
    length, _ = cotangent.shape
    n = lax.axis_size("sp")
    n_tp = lax.axis_size("tp")
    slots = 4 * length // n
    slots = (slots + ROW_TILE - 1) // ROW_TILE * ROW_TILE
    plus = jax.nn.softplus(-decay_param)
    (
        normed_grad, grad_gate, grad_up, grad_down,
        maps, decay, ones, coef_a, coef_c, coef_e, value, slope, mixed_out, tot,
    ) = front(
        (
            cotangent, saved_input, routes.T, route_weight.T, gate_proj[0], up_proj[0], down_proj[0],
            conv_input, gate_branch, conv_taps, recur_map, input_map, decay_shift,
        ),
        plus, None, n, n_tp, slots,
    )
    grad_out, input_grad, branch_grad = tail(
        (
            normed_grad, cotangent, saved_input, out_proj, decay, ones, coef_a, coef_c, coef_e,
            value, slope, maps, tot, mixed_out, conv_taps,
        ),
        n,
    )
    return (grad_gate[None], grad_up[None], grad_down[None], grad_out, input_grad, branch_grad)


def solution(mesh):
    in_specs = (
        P("sp", None),
        P("sp", None),
        P("sp", None),
        P("sp", None),
        P("sp", None, "tp"),
        P("sp", None, "tp"),
        P("sp", "tp", None),
        P(None, "tp"),
        P("sp", "tp"),
        P("sp", "tp"),
        P(None, "tp"),
        P(None, "tp", None, None),
        P(None, "tp", None, None),
        P(None, "tp"),
        P(None, "sp", "tp"),
    )
    out_specs = (
        P("sp", None, "tp"),
        P("sp", None, "tp"),
        P("sp", "tp", None),
        P("sp", "tp"),
        P("sp", "tp"),
        P("sp", "tp"),
    )
    return jax.shard_map(shards, mesh=mesh, in_specs=in_specs, out_specs=out_specs, check_vma=False)
```

```python
import functools
import jax
import jax.numpy as jnp
from jax import lax
from jax.experimental import pallas as pl
from jax.experimental.pallas import tpu as pltpu
from jax.sharding import PartitionSpec as P

EPS = 1e-06
DECAY_SCALE = 8.0
ROW_TILE = 16
LAG = 3
VMEM_LIMIT = 62 * 2**20
GELU_K = 0.7978845608028654
GELU_C = 0.044715
VM = pl.BlockSpec(memory_space=pltpu.VMEM)
HB = pl.BlockSpec(memory_space=pltpu.HBM)
BF = jnp.bfloat16
F32 = jnp.float32
ROWS0 = (((0,), (0,)), ((), ()))
COLS1 = (((1,), (1,)), ((), ()))
PLAIN = (((1,), (0,)), ((), ()))


def neighbours():
    tp = lax.axis_index("tp")
    side = tp // 2
    core = tp % 2
    return tp, side * 2 + (1 - core), (1 - side) * 2 + core, (1 - side) * 2 + (1 - core)


def partner_at(sp, n, d):
    if n & (n - 1):
        return (sp + d) % n
    bit, peer = 1, sp
    while bit < n:
        if d & bit:
            peer = peer + bit * (1 - 2 * ((sp // bit) % 2))
        bit *= 2
    return peer


def source_at(sp, n, d):
    return (sp + n - d) % n if n & (n - 1) else partner_at(sp, n, d)


def announce(n, tps):
    sp = lax.axis_index("sp")
    tp = lax.axis_index("tp")
    barrier = pltpu.get_barrier_semaphore()
    for d in range(1, n):
        pl.semaphore_signal(
            barrier, inc=1, device_id=((sp + d) % n, tp), device_id_type=pl.DeviceIdType.MESH
        )
    for other in tps:
        pl.semaphore_signal(barrier, inc=1, device_id=(sp, other), device_id_type=pl.DeviceIdType.MESH)
    return barrier, n - 1 + len(tps)


def remote(src, dst, sems, index, device):
    return pltpu.make_async_remote_copy(
        src_ref=src,
        dst_ref=dst,
        send_sem=sems.at[(0,) + index],
        recv_sem=sems.at[(1,) + index],
        device_id=device,
        device_id_type=pl.DeviceIdType.MESH,
    )


def edge_copies(n, x_ref, halo_ref, sems):
    sp = lax.axis_index("sp")
    tp = lax.axis_index("tp")
    length, tile = x_ref.shape[0], halo_ref.shape[1]
    copies = (
        remote(x_ref.at[pl.ds(length - tile, tile)], halo_ref.at[0], sems, (0,), ((sp + 1) % n, tp)),
        remote(x_ref.at[pl.ds(0, tile)], halo_ref.at[1], sems, (1,), ((sp + n - 1) % n, tp)),
    )
    for copy in copies:
        copy.start()
    return copies


def halo_rows(halo_ref, n):
    sp = lax.axis_index("sp")
    before = jnp.where(sp == 0, 0.0, halo_ref[0].astype(F32))
    after = jnp.where(sp == n - 1, 0.0, halo_ref[1].astype(F32))
    return before[before.shape[0] - 2 :], after[:2]


def split_dot(x, w, dims):
    high = x.astype(BF)
    low = (x - high.astype(F32)).astype(BF)
    total = lax.dot_general(low, w, dims, preferred_element_type=F32)
    return total + lax.dot_general(high, w, dims, preferred_element_type=F32)


def minus_expm1(y):
    series = 1.0 + y * (1.0 / 8.0)
    for k in (7.0, 6.0, 5.0, 4.0, 3.0, 2.0):
        series = 1.0 + y * (1.0 / k) * series
    return jnp.where(y > -0.25, -y * series, 1.0 - jnp.exp(y))


def softplus(x):
    u = jnp.exp(-jnp.abs(x))
    series = 1.0 / 9.0
    for k in (8.0, 7.0, 6.0, 5.0, 4.0, 3.0, 2.0, 1.0):
        series = 1.0 / k - u * series
    return jnp.maximum(x, 0.0) + jnp.where(u < 0.05, u * series, jnp.log(1.0 + u))


def shifted(x, by, edge):
    length = x.shape[0]
    row = lax.broadcasted_iota(jnp.int32, x.shape, 0)
    moved = pltpu.roll(x, by % length, 0)
    return jnp.where(row == (0 if by > 0 else length - 1), edge, moved)


def run_scans(length, jobs):
    width = jobs[0][1].shape[1]
    groups = length // 8

    def body(g, carry):
        out = []
        for (reverse, a_ref, b_ref, to_ref), state in zip(jobs, carry):
            base = pl.multiple_of((groups - 1 - g if reverse else g) * 8, 8)
            a = a_ref[pl.ds(base, 8), :]
            b = None if b_ref is None else b_ref[pl.ds(base, 8), :]
            rows = [None] * 8
            for k in reversed(range(8)) if reverse else range(8):
                state = a[k : k + 1] * state
                if b is not None:
                    state = state + b[k : k + 1]
                rows[k] = state
            to_ref[pl.ds(base, 8), :] = jnp.concatenate(rows, axis=0)
            out.append(state)
        return tuple(out)

    start = tuple(
        jnp.full((1, width), 1.0 if b_ref is None else 0.0, F32) for _, _, b_ref, _ in jobs
    )
    return lax.fori_loop(0, groups, body, start)


def gelu_parts(x):
    t = jnp.tanh(GELU_K * (x + GELU_C * x * x * x))
    value = 0.5 * x * (1.0 + t)
    slope = 0.5 * (1.0 + t) + 0.5 * x * (1.0 - t * t) * GELU_K * (1.0 + 3.0 * GELU_C * x * x)
    return value, slope


def carries(n, all_ref, rows):
    sp = lax.axis_index("sp")
    zero = jnp.zeros((1, all_ref.shape[2]), F32)
    (lp, le), (up, ue) = rows

    def lower(k, carry):
        t = all_ref[k]
        return t[lp : lp + 1] * carry + t[le : le + 1]

    def upper(i, carry):
        t = all_ref[n - 1 - i]
        return t[up : up + 1] * carry + t[ue : ue + 1]

    return lax.fori_loop(0, sp, lower, zero), lax.fori_loop(0, n - 1 - sp, upper, zero)


def whole_kernel(n, slots, *refs):
    (
        cot_hbm, x_hbm, routes_hbm, weight_hbm, wg_hbm, wu_hbm, wd_hbm, proj_hbm, cin_hbm,
        branch_hbm, taps_hbm, rmap_hbm, imap_hbm, param_hbm, shift_hbm,
        ggate_hbm, gup_hbm, gdown_hbm, grad_out_hbm, input_grad_hbm, branch_grad_hbm,
        routes_ref, weight_ref, cin_ref, branch_ref, taps_ref, rmap_ref, imap_ref, param_ref,
        cot_ref, x_ref, nx_ref, wg_ref, wu_ref, wd_ref, proj_ref, shift_ref,
        ng_ref, ggate_ref, gup_ref, gdown_ref, grad_out_ref, input_grad_ref, branch_grad_ref,
        pick_ref, send_ref, rows_sc, rows_in, hid_ref, ggu_ref, part_ref,
        got1, got2, mid, fin, back, halo_ref,
        maps_ref, decay_ref, ones_ref, a_ref, c_ref, e_ref, value_ref, slope_ref, tot_ref,
        conv_ref, gates_ref, root_ref, drive_ref, state_ref, cum_ref, all_ref,
        mixed_ref, mixed_all, out_all, after_ref, msg_ref, every_ref, conv_grad_ref, halo2_ref,
        loc, put, edge, hop, pair, cross, fwd, s_pair, s_cross, s_hop, s_tail, s_tot,
        s_msg, s_mix, s_share, s_out, s_edge,
    ) = refs
    length, width = cot_ref.shape
    fourth = send_ref.shape[3]
    channels = cin_ref.shape[1]
    sp = lax.axis_index("sp")
    tp, partner, across, diagonal = neighbours()
    unit = n // 8
    rows = (rows_sc, rows_in)

    def cols(q):
        return pl.ds(pl.multiple_of(q * fourth, 128), fourth)

    loads = [
        pltpu.make_async_copy(src, dst, loc.at[i])
        for i, (src, dst) in enumerate(
            (
                (x_hbm, x_ref), (cot_hbm, cot_ref), (shift_hbm, shift_ref),
                (wg_hbm, wg_ref), (wu_hbm, wu_ref), (wd_hbm, wd_ref), (proj_hbm, proj_ref),
                (cin_hbm, cin_ref), (routes_hbm, routes_ref), (weight_hbm, weight_ref),
                (taps_hbm, taps_ref), (rmap_hbm, rmap_ref), (imap_hbm, imap_ref),
                (param_hbm, param_ref), (branch_hbm, branch_ref),
            )
        )
    ]
    for i in (8, 9, 0, 1, 7, 10, 11, 12, 13, 2, 14, 3, 4, 5, 6):
        loads[i].start()

    barrier, heard = announce(n, (partner, across))
    puts = []

    def store(src, dst):
        copy = pltpu.make_async_copy(src, dst, put.at[len(puts)])
        copy.start()
        puts.append(copy)

    loads[8].wait()
    loads[9].wait()
    route0, route1 = routes_ref[0:1], routes_ref[1:2]
    offset = lax.broadcasted_iota(jnp.int32, (n, length), 0)
    which = (offset + sp) % n if n & (n - 1) else offset ^ sp
    first, second = which == route0, which == route1
    named = (first | second).astype(F32).astype(BF)
    earlier = lax.broadcasted_iota(jnp.int32, (length, length), 0) < lax.broadcasted_iota(
        jnp.int32, (length, length), 1
    )
    rank = jnp.dot(named, earlier.astype(F32).astype(BF), preferred_element_type=F32)
    place = (offset * slots).astype(F32) + rank
    target0 = jnp.sum(jnp.where(first, place, 0.0), axis=0, keepdims=True).astype(jnp.int32)
    target1 = jnp.sum(jnp.where(second, place, 0.0), axis=0, keepdims=True).astype(jnp.int32)
    loads[0].wait()
    for r in range(0, length, 32):
        x = x_ref[r : r + 32].astype(F32)
        inv = lax.rsqrt(jnp.mean(x * x, axis=1, keepdims=True) + EPS)
        nx_ref[r : r + 32] = (x * inv).astype(BF)

    def chosen(lo, hi):
        slot = lax.broadcasted_iota(jnp.int32, ((hi - lo) * slots, length), 0) + lo * slots
        hit0, hit1 = slot == target0, slot == target1
        pick = (hit0 | hit1).astype(F32).astype(BF)
        pick_ref[lo * slots : hi * slots] = pick
        share = jnp.where(hit0, weight_ref[0:1], 0.0) + jnp.where(hit1, weight_ref[1:2], 0.0)
        return pick, jnp.sum(share, axis=1, keepdims=True)

    def taken(pick, share, where):
        cot = jnp.dot(pick, cot_ref[:, where], preferred_element_type=F32)
        got = jnp.dot(pick, nx_ref[:, where], preferred_element_type=F32).astype(BF)
        return (cot * share).astype(BF), got

    order = [
        d for lo, hi in ((1, 4 * unit), (6 * unit, n), (4 * unit, 6 * unit)) for d in range(lo, hi)
    ]
    hops = {}
    loads[1].wait()
    for lo, hi in ((0, 4 * unit), (4 * unit, n)):
        pick, share = chosen(lo, hi)
        for a, value in enumerate(taken(pick, share, cols(tp))):
            send_ref[a, lo:hi] = value.reshape(hi - lo, slots, fourth)
        if lo == 0:
            own = pick[:slots], share[:slots]
            pl.semaphore_wait(barrier, heard)
            loads[7].wait()
            edges = edge_copies(n, cin_ref, halo_ref, edge)
        for d in order:
            if lo <= d < hi:
                for a in range(2):
                    copy = remote(
                        send_ref.at[a, d], rows[a].at[d, :, cols(tp)], hop, (a, d),
                        (partner_at(sp, n, d), tp),
                    )
                    copy.start()
                    hops[a, d] = copy
    for q in range(width // fourth):
        where = pl.ds(q * fourth, fourth)
        rows_sc[0, :, where], rows_in[0, :, where] = taken(*own, where)

    for i in (10, 11, 12, 13):
        loads[i].wait()
    plus = softplus(-param_ref[...])
    heads, hw = rmap_ref.shape[1], rmap_ref.shape[2]
    spread = (
        lax.broadcasted_iota(jnp.int32, (hw, channels), 1) % hw
        == lax.broadcasted_iota(jnp.int32, (hw, channels), 0)
    ).astype(F32).astype(BF)
    block = (
        lax.broadcasted_iota(jnp.int32, (channels, channels), 0) // hw
        == lax.broadcasted_iota(jnp.int32, (channels, channels), 1) // hw
    )
    for i in range(4):
        stack = (rmap_ref, imap_ref)[i % 2][i // 2].reshape(heads * hw, hw)
        full = jnp.dot(stack, spread, preferred_element_type=F32)
        maps_ref[:, i * channels : (i + 1) * channels] = jnp.where(block, full, 0.0).astype(BF)
    for copy in edges:
        copy.wait()
    taps = taps_ref[...].astype(F32)
    low, high = halo_rows(halo_ref, n)
    x = cin_ref[...].astype(F32)
    back1 = shifted(x, 1, low[1:2])
    back2 = shifted(back1, 1, low[0:1])
    conv = back2 * taps[0:1] + back1 * taps[1:2] + x * taps[2:3]
    conv = conv + shifted(x, -1, high[0:1]) * taps[3:4]
    conv_ref[...] = conv
    gates_ref[...] = jax.nn.sigmoid(split_dot(conv, maps_ref[...], PLAIN))
    loads[2].wait()
    for d in range(2):
        recur = gates_ref[:, 2 * d * channels : (2 * d + 1) * channels]
        inputs = gates_ref[:, (2 * d + 1) * channels : (2 * d + 2) * channels]
        log_decay = -DECAY_SCALE * recur * plus[d : d + 1] + shift_ref[d]
        root = jnp.sqrt(minus_expm1(2.0 * log_decay))
        decay_ref[d] = jnp.exp(log_decay)
        root_ref[d] = root
        drive_ref[d] = root * (inputs * conv_ref[...])
    a_f, a_b = decay_ref.at[0], decay_ref.at[1]
    ends = run_scans(
        length,
        (
            (False, a_f, drive_ref.at[0], state_ref.at[0]),
            (True, a_b, drive_ref.at[1], state_ref.at[1]),
            (False, a_f, None, cum_ref.at[0]),
            (True, a_b, None, cum_ref.at[1]),
            (True, a_f, None, ones_ref.at[0]),
            (False, a_b, None, ones_ref.at[1]),
        ),
    )
    tot_ref[0:1, :] = ends[2]
    tot_ref[1:2, :] = ends[0]
    tot_ref[2:3, :] = ends[3]
    tot_ref[3:4, :] = ends[1]
    tot_ref[4:8, :] = jnp.zeros((4, channels), F32)
    totals = []
    for d in range(n - 1, 0, -1):
        copy = remote(tot_ref, all_ref.at[sp], s_tot, (d,), (partner_at(sp, n, d), tp))
        copy.start()
        totals.append(copy)
    all_ref[sp] = tot_ref[...]

    def finish_states():
        for copy in totals:
            copy.wait()
        in_f, in_b = carries(n, all_ref, ((0, 1), (2, 3)))
        state_f = state_ref[0] + cum_ref[0] * in_f
        state_b = state_ref[1] + cum_ref[1] * in_b
        beside = (shifted(state_f, 1, in_f), shifted(state_b, -1, in_b))
        loads[14].wait()
        value, slope = gelu_parts(branch_ref[...].astype(F32))
        states = state_f + state_b
        value_ref[...] = value
        slope_ref[...] = states * slope
        out_all[0] = (value * states).astype(BF)
        conv = conv_ref[...]
        for d in range(2):
            recur = gates_ref[:, 2 * d * channels : (2 * d + 1) * channels]
            inputs = gates_ref[:, (2 * d + 1) * channels : (2 * d + 2) * channels]
            decay = decay_ref[d]
            root = root_ref[d]
            a_ref[d] = root * inputs
            g_log = beside[d] * decay - inputs * conv * (decay * decay) / root
            c_ref[d] = g_log * (-DECAY_SCALE * plus[d : d + 1]) * recur * (1.0 - recur)
            e_ref[d] = root * conv * inputs * (1.0 - inputs)

    nears, fwds, overs, late = {}, {}, {}, []

    def step_in(a, d):
        hops[a, d].wait_recv()
        dst = rows[a]
        mine = dst.at[d, :, cols(tp)]
        overs[a, d] = remote(mine, mine, cross, (a, d), (sp, across))
        overs[a, d].start()
        late.append((a, d))
        nears[a, d] = remote(mine, mine, pair, (a, d), (sp, partner))
        nears[a, d].start()

    def step_on():
        a, d = late.pop(0)
        overs[a, d].wait_recv()
        other = rows[a].at[d, :, cols(across)]
        fwds[a, d] = remote(other, other, fwd, (a, d), (sp, partner))
        fwds[a, d].start()

    def bring(lo, hi):
        for d in order:
            if lo * unit <= d < hi * unit:
                for a in range(2):
                    step_in(a, d)
                    if len(late) > LAG:
                        step_on()

    pairs, crosses, backs = {}, {}, {}

    def experts(lo, hi):
        lo, hi = lo * unit, hi * unit
        while any(lo <= d < hi for _, d in late):
            step_on()
        for d in range(lo, hi):
            if d:
                for a in range(2):
                    nears[a, d].wait_recv()
                    fwds[a, d].wait_recv()
        count = (hi - lo) * slots
        at = slice(lo * slots, hi * slots)
        xin = rows_in[lo:hi].reshape(count, width)
        gate_pre = jnp.dot(xin, wg_ref[...], preferred_element_type=F32)
        up_pre = jnp.dot(xin, wu_ref[...], preferred_element_type=F32)
        xsc = rows_sc[lo:hi].reshape(count, width)
        hidden_grad = lax.dot_general(xsc, wd_ref[...], COLS1, preferred_element_type=F32)
        gate_sig = jax.nn.sigmoid(gate_pre)
        gate_act = gate_pre * gate_sig
        hid_ref[at] = (gate_act * up_pre).astype(BF)
        gate_grad = hidden_grad * up_pre * gate_sig * (1.0 + gate_pre * (1.0 - gate_sig))
        gate_grad = gate_grad.astype(BF)
        up_grad = (hidden_grad * gate_act).astype(BF)
        units = up_grad.shape[1]
        ggu_ref[at, :units] = gate_grad
        ggu_ref[at, units:] = up_grad
        for i, q in enumerate((diagonal, partner, across, tp)):
            some = pl.ds(pl.multiple_of(q * fourth, 128), fourth)
            total = lax.dot_general(gate_grad, wg_ref[some], COLS1, preferred_element_type=F32)
            total = total + lax.dot_general(up_grad, wu_ref[some], COLS1, preferred_element_type=F32)
            part_ref[lo:hi, :, cols(q)] = total.astype(BF).reshape(hi - lo, slots, fourth)
            if i < 2:
                for d in range(lo, hi):
                    copy = remote(
                        part_ref.at[d, :, cols(q)], got1.at[i, d], s_pair, (i, d), (sp, partner)
                    )
                    copy.start()
                    pairs[i, d] = copy

    def stage_b(lo, hi):
        for d in range(lo * unit, hi * unit):
            pairs[0, d].wait_recv()
            total = part_ref[d, :, cols(across)].astype(F32) + got1[0, d].astype(F32)
            mid[d] = total.astype(BF)
            crosses[d] = remote(mid.at[d], got2.at[d], s_cross, (d,), (sp, across))
            crosses[d].start()

    def stage_c(lo, hi):
        for d in range(lo * unit, hi * unit):
            pairs[1, d].wait_recv()
            crosses[d].wait_recv()
            total = part_ref[d, :, cols(tp)].astype(F32) + got1[1, d].astype(F32)
            total = (total + got2[d].astype(F32)).astype(BF)
            if d == 0:
                back[0] = total
            else:
                fin[d] = total
                backs[d] = remote(fin.at[d], back.at[d], s_hop, (d,), (source_at(sp, n, d), tp))
                backs[d].start()

    chunk = width // 8

    def weight_gradients(k):
        at = slice(k * chunk, (k + 1) * chunk)
        units = hid_ref.shape[1]
        left = rows_in[:, :, at].reshape(n * slots, chunk)
        both = lax.dot_general(left, ggu_ref[...], ROWS0, preferred_element_type=F32)
        ggate_ref[at] = both[:, :units]
        gup_ref[at] = both[:, units:]
        right = rows_sc[:, :, at].reshape(n * slots, chunk)
        gdown_ref[:, at] = lax.dot_general(hid_ref[...], right, ROWS0, preferred_element_type=F32)
        store(ggate_ref.at[at], ggate_hbm.at[at])
        store(gup_ref.at[at], gup_hbm.at[at])
        store(gdown_ref.at[:, at], gdown_hbm.at[:, at])

    powers = n & (n - 1) == 0
    bits = [n >> i for i in range(1, n.bit_length())] if powers else []
    gathers = []

    def gather(pairs_of):
        got = []
        for d, to, hop_to in pairs_of:
            copy = remote(out_all.at[d], out_all.at[to], s_out, (to,), (partner_at(sp, n, hop_to), tp))
            copy.start()
            got.append(copy)
        gathers.append(got)

    def gather_start():
        if powers:
            bit = bits.pop(0)
            gather([(d, d + bit, bit) for d in range(0, n, 2 * bit)])
        else:
            gather([(0, d, d) for d in range(1, n)])

    def gather_on():
        if bits:
            for copy in gathers[-1]:
                copy.wait_recv()
            gather_start()

    bring(0, 2)
    bring(2, 4)
    for i in (3, 4, 5):
        loads[i].wait()
    experts(0, 2)
    bring(6, 8)
    experts(2, 4)
    bring(4, 6)
    experts(6, 8)
    stage_b(6, 8)
    experts(4, 6)
    stage_c(6, 8)
    stage_b(4, 6)
    stage_b(2, 4)
    stage_c(4, 6)
    stage_b(0, 2)
    stage_c(2, 4)
    stage_c(0, 2)
    finish_states()
    weight_gradients(0)
    gather_start()
    for k in range(1, 8):
        weight_gradients(k)
    for d in range(1, n):
        backs[d].wait_recv()
    got = back[...].reshape(n * slots, fourth)
    grad = lax.dot_general(pick_ref[...], got, ROWS0, preferred_element_type=F32)
    ng_ref[:, cols(tp)] = grad.astype(BF)
    own = ng_ref.at[:, cols(tp)]
    over = remote(own, own, s_tail, (0,), (sp, across))
    near = remote(own, own, s_tail, (1,), (sp, partner))
    over.start()
    near.start()
    over.wait_recv()
    other = ng_ref.at[:, cols(across)]
    last = remote(other, other, s_tail, (2,), (sp, partner))
    last.start()
    gather_on()
    for group in (hops, nears, fwds, overs, pairs, crosses, backs):
        for copy in group.values():
            copy.wait_send()
    near.wait()
    over.wait_send()
    last.wait()

    part = width // n
    half = length // 2
    mine = pl.ds(pl.multiple_of((tp % 2) * half, ROW_TILE), half)
    for r in range(0, length, 32):
        x = x_ref[r : r + 32].astype(F32)
        inv = lax.rsqrt(jnp.mean(x * x, axis=1, keepdims=True) + EPS)
        normed = x * inv
        ng = ng_ref[r : r + 32].astype(F32)
        dot = jnp.mean(ng * normed, axis=1, keepdims=True)
        mixed = (cot_ref[r : r + 32].astype(F32) + inv * (ng - normed * dot)).astype(BF)
        for e in range(n):
            mixed_ref[e, r : r + 32] = mixed[:, e * part : (e + 1) * part]
    mixes, shares = {}, {}

    def mix(ds):
        for d in ds:
            peer = partner_at(sp, n, d)
            mixes[d] = remote(
                mixed_ref.at[peer, mine], mixed_all.at[d, mine], s_mix, (d,), (peer, tp)
            )
            mixes[d].start()

    reach = order[::-1]
    early = reach[: 2 * unit]
    mix(early)
    loads[6].wait()
    out_grad = jnp.zeros((length, channels), F32)
    for e in range(n):
        out_grad = out_grad + jnp.dot(
            mixed_ref[e], proj_ref[e * part : (e + 1) * part], preferred_element_type=F32
        )
    carried = out_grad * value_ref[...]
    branch_grad_ref[...] = (out_grad * slope_ref[...]).astype(BF)
    store(branch_grad_ref, branch_grad_hbm)
    drive_ref[...] = decay_ref[...] * carried[None]
    ends = run_scans(
        length,
        (
            (True, decay_ref.at[0], drive_ref.at[0], after_ref.at[0]),
            (False, decay_ref.at[1], drive_ref.at[1], after_ref.at[1]),
        ),
    )
    msg_ref[0:1, :] = tot_ref[0:1, :]
    msg_ref[1:2, :] = tot_ref[2:3, :]
    msg_ref[2:3, :] = ends[1]
    msg_ref[3:4, :] = ends[0]
    msg_ref[4:8, :] = jnp.zeros((4, channels), F32)
    sums = []
    for d in range(n - 1, 0, -1):
        copy = remote(msg_ref, every_ref.at[sp], s_msg, (d,), (partner_at(sp, n, d), tp))
        copy.start()
        sums.append(copy)
    every_ref[sp] = msg_ref[...]
    mix([d for d in reach if d not in early])
    mixed_all[0] = mixed_ref[sp]
    gather_on()
    for copy in sums:
        copy.wait()
    in_ab, in_af = carries(n, every_ref, ((1, 2), (0, 3)))
    after_f = after_ref[0] + ones_ref[0] * in_af
    after_b = after_ref[1] + ones_ref[1] * in_ab
    adjoint = (carried + shifted(after_f, -1, in_af), carried + shifted(after_b, 1, in_ab))
    total = adjoint[0] * a_ref[0] + adjoint[1] * a_ref[1]
    for d in range(2):
        gates_ref[:, 2 * d * channels : (2 * d + 1) * channels] = adjoint[d] * c_ref[d]
        gates_ref[:, (2 * d + 1) * channels : (2 * d + 2) * channels] = adjoint[d] * e_ref[d]
    total = total + split_dot(gates_ref[...], maps_ref[...], COLS1)
    conv_grad_ref[...] = total.astype(BF)
    rims = edge_copies(n, conv_grad_ref, halo2_ref, s_edge)
    while bits:
        gather_on()
    for d in reach:
        mixes[d].wait_recv()
        block = mixed_all.at[d, mine]
        shares[d] = remote(block, block, s_share, (d,), (sp, partner))
        shares[d].start()
    for copy in rims:
        copy.wait()
    taps = taps_ref[...].astype(F32)
    low, high = halo_rows(halo2_ref, n)
    up1 = shifted(total, -1, high[0:1])
    up2 = shifted(up1, -1, high[1:2])
    down = shifted(total, 1, low[1:2])
    result = up2 * taps[0:1] + up1 * taps[1:2] + total * taps[2:3] + down * taps[3:4]
    input_grad_ref[...] = result.astype(BF)
    store(input_grad_ref, input_grad_hbm)
    for d in range(1, n):
        shares[d].wait()
        mixes[d].wait_send()
    for got in gathers[:-1]:
        for copy in got:
            copy.wait_send()
    for copy in gathers[-1]:
        copy.wait()
    grad_out_ref[...] = lax.dot_general(
        mixed_all[...].reshape(n * length, part),
        out_all[...].reshape(n * length, channels),
        ROWS0,
        preferred_element_type=F32,
    )
    store(grad_out_ref, grad_out_hbm)
    for copy in puts:
        copy.wait()


def whole(args, n, n_tp, slots):
    cot, wg, proj, cin = args[0], args[4], args[7], args[8]
    length, width = cot.shape
    channels = cin.shape[1]
    units = wg.shape[1]
    fourth = width // n_tp
    part = width // n
    dma = pltpu.SemaphoreType.DMA
    sds = jax.ShapeDtypeStruct
    vm = pltpu.VMEM
    one, two = (length, channels), (2, length, channels)
    outs = (
        sds((width, units), F32),
        sds((width, units), F32),
        sds((units, width), F32),
        sds((part, channels), F32),
        sds(one, BF),
        sds(one, BF),
    )
    block = (n, slots, fourth)
    scratch = [
        *(vm(args[i].shape, args[i].dtype) for i in (2, 3, 8, 9, 10, 11, 12, 13)),
        vm((length, width), BF), vm((length, width), BF), vm((length, width), BF),
        vm((width, units), BF), vm((width, units), BF), vm((units, width), BF),
        vm(proj.shape, BF), vm(two, F32),
        vm((length, width), BF),
        *(vm(out.shape, out.dtype) for out in outs),
        vm((n * slots, length), BF), vm((2,) + block, BF),
        vm((n, slots, width), BF), vm((n, slots, width), BF),
        vm((n * slots, units), BF), vm((n * slots, 2 * units), BF), vm((n, slots, width), BF),
        vm((2,) + block, BF), vm(block, BF), vm(block, BF), vm(block, BF), vm(block, BF),
        vm((2, ROW_TILE, channels), BF),
        vm((channels, 4 * channels), BF),
        vm(two, F32), vm(two, F32), vm(two, F32), vm(two, F32), vm(two, F32),
        vm(one, F32), vm(one, F32), vm((8, channels), F32),
        vm(one, F32), vm((length, 4 * channels), F32), vm(two, F32), vm(two, F32), vm(two, F32),
        vm(two, F32), vm((n, 8, channels), F32),
        vm((n, length, part), BF), vm((n, length, part), BF), vm((n, length, channels), BF),
        vm(two, F32), vm((8, channels), F32), vm((n, 8, channels), F32),
        vm((length, channels), BF), vm((2, ROW_TILE, channels), BF),
        dma((15,)), dma((3 * 8 + 3,)),
        dma((2, 2)), dma((2, 2, n)), dma((2, 2, n)), dma((2, 2, n)),
        dma((2, 2, n)), dma((2, 2, n)), dma((2, n)), dma((2, n)), dma((2, 3)), dma((2, n)),
        dma((2, n)), dma((2, n)), dma((2, n)), dma((2, n)), dma((2, 2)),
    ]
    return pl.pallas_call(
        functools.partial(whole_kernel, n, slots),
        out_shape=outs,
        in_specs=[HB] * len(args),
        out_specs=[HB] * len(outs),
        scratch_shapes=scratch,
        compiler_params=pltpu.CompilerParams(
            collective_id=1, has_side_effects=True, vmem_limit_bytes=VMEM_LIMIT
        ),
        cost_estimate=pl.CostEstimate(
            flops=2_000_000_000, bytes_accessed=30_000_000, transcendentals=0
        ),
    )(*args)


def written(*arrays):
    count = len(arrays)
    cuts = [8 if x.size * x.dtype.itemsize > 2**20 else 1 for x in arrays]
    offsets = [sum(cuts[:i]) for i in range(count)]

    def kernel(*refs):
        sems = refs[-1]
        sets = []
        for i in range(count):
            src, dst, held = refs[i], refs[count + i], refs[2 * count + i]
            step = src.shape[0] // cuts[i]
            for k in range(cuts[i]):
                at = pl.ds(k * step, step)
                j = offsets[i] + k
                inward = pltpu.make_async_copy(src.at[at], held.at[at], sems.at[0, j])
                outward = pltpu.make_async_copy(held.at[at], dst.at[at], sems.at[1, j])
                inward.start()
                sets.append((inward, outward))
        for inward, outward in sets:
            inward.wait()
            outward.start()
        for _, outward in sets:
            outward.wait()

    return pl.pallas_call(
        kernel,
        out_shape=tuple(jax.ShapeDtypeStruct(x.shape, x.dtype) for x in arrays),
        in_specs=[HB] * count,
        out_specs=[HB] * count,
        scratch_shapes=[pltpu.VMEM(x.shape, x.dtype) for x in arrays]
        + [pltpu.SemaphoreType.DMA((2, sum(cuts)))],
        compiler_params=pltpu.CompilerParams(vmem_limit_bytes=VMEM_LIMIT),
    )(*arrays)


def shards(
    cotangent,
    saved_input,
    routes,
    route_weight,
    gate_proj,
    up_proj,
    down_proj,
    out_proj,
    conv_input,
    gate_branch,
    conv_taps,
    recur_map,
    input_map,
    decay_param,
    decay_shift,
):
    length, _ = cotangent.shape
    n = lax.axis_size("sp")
    n_tp = lax.axis_size("tp")
    slots = 4 * length // n
    slots = (slots + ROW_TILE - 1) // ROW_TILE * ROW_TILE
    grad_gate, grad_up, grad_down, *others = written(
        *whole(
            (
                cotangent, saved_input, routes.T, route_weight.T, gate_proj[0], up_proj[0],
                down_proj[0], out_proj, conv_input, gate_branch, conv_taps, recur_map, input_map,
                decay_param, decay_shift,
            ),
            n, n_tp, slots,
        )
    )
    return (grad_gate[None], grad_up[None], grad_down[None], *others)


def solution(mesh):
    in_specs = (
        P("sp", None),
        P("sp", None),
        P("sp", None),
        P("sp", None),
        P("sp", None, "tp"),
        P("sp", None, "tp"),
        P("sp", "tp", None),
        P(None, "tp"),
        P("sp", "tp"),
        P("sp", "tp"),
        P(None, "tp"),
        P(None, "tp", None, None),
        P(None, "tp", None, None),
        P(None, "tp"),
        P(None, "sp", "tp"),
    )
    out_specs = (
        P("sp", None, "tp"),
        P("sp", None, "tp"),
        P("sp", "tp", None),
        P("sp", "tp"),
        P("sp", "tp"),
        P("sp", "tp"),
    )
    return jax.shard_map(shards, mesh=mesh, in_specs=in_specs, out_specs=out_specs, check_vma=False)
```

```python
import functools
import jax
import jax.numpy as jnp
from jax import lax
from jax.experimental import pallas as pl
from jax.experimental.pallas import tpu as pltpu
from jax.sharding import PartitionSpec as P

EPS = 1e-06
DECAY_SCALE = 8.0
ROW_TILE = 16
LAG = 3
VMEM_LIMIT = 62 * 2**20
GELU_K = 0.7978845608028654
GELU_C = 0.044715
VM = pl.BlockSpec(memory_space=pltpu.VMEM)
HB = pl.BlockSpec(memory_space=pltpu.HBM)
BF = jnp.bfloat16
F32 = jnp.float32
ROWS0 = (((0,), (0,)), ((), ()))
COLS1 = (((1,), (1,)), ((), ()))
PLAIN = (((1,), (0,)), ((), ()))


def neighbours():
    tp = lax.axis_index("tp")
    side = tp // 2
    core = tp % 2
    return tp, side * 2 + (1 - core), (1 - side) * 2 + core, (1 - side) * 2 + (1 - core)


def partner_at(sp, n, d):
    if n & (n - 1):
        return (sp + d) % n
    bit, peer = 1, sp
    while bit < n:
        if d & bit:
            peer = peer + bit * (1 - 2 * ((sp // bit) % 2))
        bit *= 2
    return peer


def source_at(sp, n, d):
    return (sp + n - d) % n if n & (n - 1) else partner_at(sp, n, d)


def announce(n, tps):
    sp = lax.axis_index("sp")
    tp = lax.axis_index("tp")
    barrier = pltpu.get_barrier_semaphore()
    for d in range(1, n):
        pl.semaphore_signal(
            barrier, inc=1, device_id=((sp + d) % n, tp), device_id_type=pl.DeviceIdType.MESH
        )
    for other in tps:
        pl.semaphore_signal(barrier, inc=1, device_id=(sp, other), device_id_type=pl.DeviceIdType.MESH)
    return barrier, n - 1 + len(tps)


def remote(src, dst, sems, index, device):
    return pltpu.make_async_remote_copy(
        src_ref=src,
        dst_ref=dst,
        send_sem=sems.at[(0,) + index],
        recv_sem=sems.at[(1,) + index],
        device_id=device,
        device_id_type=pl.DeviceIdType.MESH,
    )


def edge_copies(n, x_ref, halo_ref, sems):
    sp = lax.axis_index("sp")
    tp = lax.axis_index("tp")
    length, tile = x_ref.shape[0], halo_ref.shape[1]
    copies = (
        remote(x_ref.at[pl.ds(length - tile, tile)], halo_ref.at[0], sems, (0,), ((sp + 1) % n, tp)),
        remote(x_ref.at[pl.ds(0, tile)], halo_ref.at[1], sems, (1,), ((sp + n - 1) % n, tp)),
    )
    for copy in copies:
        copy.start()
    return copies


def halo_rows(halo_ref, n):
    sp = lax.axis_index("sp")
    before = jnp.where(sp == 0, 0.0, halo_ref[0].astype(F32))
    after = jnp.where(sp == n - 1, 0.0, halo_ref[1].astype(F32))
    return before[before.shape[0] - 2 :], after[:2]


def split_dot(x, w, dims):
    high = x.astype(BF)
    low = (x - high.astype(F32)).astype(BF)
    total = lax.dot_general(low, w, dims, preferred_element_type=F32)
    return total + lax.dot_general(high, w, dims, preferred_element_type=F32)


def minus_expm1(y):
    series = 1.0 + y * (1.0 / 8.0)
    for k in (7.0, 6.0, 5.0, 4.0, 3.0, 2.0):
        series = 1.0 + y * (1.0 / k) * series
    return jnp.where(y > -0.25, -y * series, 1.0 - jnp.exp(y))


def softplus(x):
    u = jnp.exp(-jnp.abs(x))
    series = 1.0 / 9.0
    for k in (8.0, 7.0, 6.0, 5.0, 4.0, 3.0, 2.0, 1.0):
        series = 1.0 / k - u * series
    return jnp.maximum(x, 0.0) + jnp.where(u < 0.05, u * series, jnp.log(1.0 + u))


def shifted(x, by, edge):
    length = x.shape[0]
    row = lax.broadcasted_iota(jnp.int32, x.shape, 0)
    moved = pltpu.roll(x, by % length, 0)
    return jnp.where(row == (0 if by > 0 else length - 1), edge, moved)


def run_scans(length, jobs):
    width = jobs[0][1].shape[1]
    groups = length // 8

    def body(g, carry):
        out = []
        for (reverse, a_ref, b_ref, to_ref), state in zip(jobs, carry):
            base = pl.multiple_of((groups - 1 - g if reverse else g) * 8, 8)
            a = a_ref[pl.ds(base, 8), :]
            b = None if b_ref is None else b_ref[pl.ds(base, 8), :]
            rows = [None] * 8
            for k in reversed(range(8)) if reverse else range(8):
                state = a[k : k + 1] * state
                if b is not None:
                    state = state + b[k : k + 1]
                rows[k] = state
            to_ref[pl.ds(base, 8), :] = jnp.concatenate(rows, axis=0)
            out.append(state)
        return tuple(out)

    start = tuple(
        jnp.full((1, width), 1.0 if b_ref is None else 0.0, F32) for _, _, b_ref, _ in jobs
    )
    return lax.fori_loop(0, groups, body, start)


def gelu_parts(x):
    t = jnp.tanh(GELU_K * (x + GELU_C * x * x * x))
    value = 0.5 * x * (1.0 + t)
    slope = 0.5 * (1.0 + t) + 0.5 * x * (1.0 - t * t) * GELU_K * (1.0 + 3.0 * GELU_C * x * x)
    return value, slope


def carries(n, all_ref, rows):
    sp = lax.axis_index("sp")
    zero = jnp.zeros((1, all_ref.shape[2]), F32)
    (lp, le), (up, ue) = rows

    def lower(k, carry):
        t = all_ref[k]
        return t[lp : lp + 1] * carry + t[le : le + 1]

    def upper(i, carry):
        t = all_ref[n - 1 - i]
        return t[up : up + 1] * carry + t[ue : ue + 1]

    return lax.fori_loop(0, sp, lower, zero), lax.fori_loop(0, n - 1 - sp, upper, zero)


def whole_kernel(n, slots, *refs):
    (
        cot_hbm, x_hbm, routes_hbm, weight_hbm, wg_hbm, wu_hbm, wd_hbm, proj_hbm, cin_hbm,
        branch_hbm, taps_hbm, rmap_hbm, imap_hbm, param_hbm, shift_hbm,
        ggate_hbm, gup_hbm, gdown_hbm, grad_out_hbm, input_grad_hbm, branch_grad_hbm,
        routes_ref, weight_ref, cin_ref, branch_ref, taps_ref, rmap_ref, imap_ref, param_ref,
        cot_ref, x_ref, nx_ref, wg_ref, wu_ref, wd_ref, proj_ref, shift_ref,
        ng_ref, ggate_ref, gup_ref, gdown_ref, grad_out_ref, input_grad_ref, branch_grad_ref,
        pick_ref, send_ref, rows_sc, rows_in, hid_ref, ggu_ref, part_ref,
        got1, got2, mid, fin, back, halo_ref,
        maps_ref, decay_ref, ones_ref, a_ref, c_ref, e_ref, value_ref, slope_ref, tot_ref,
        conv_ref, gates_ref, root_ref, drive_ref, state_ref, cum_ref, all_ref,
        mixed_ref, mixed_all, out_all, after_ref, msg_ref, every_ref, conv_grad_ref, halo2_ref,
        loc, put, edge, hop, pair, cross, fwd, s_pair, s_cross, s_hop, s_tail, s_tot,
        s_msg, s_mix, s_share, s_out, s_edge,
    ) = refs
    length, width = cot_ref.shape
    fourth = send_ref.shape[3]
    channels = cin_ref.shape[1]
    sp = lax.axis_index("sp")
    tp, partner, across, diagonal = neighbours()
    unit = n // 8
    rows = (rows_sc, rows_in)

    def cols(q):
        return pl.ds(pl.multiple_of(q * fourth, 128), fourth)

    loads = [
        pltpu.make_async_copy(src, dst, loc.at[i])
        for i, (src, dst) in enumerate(
            (
                (x_hbm, x_ref), (cot_hbm, cot_ref), (shift_hbm, shift_ref),
                (wg_hbm, wg_ref), (wu_hbm, wu_ref), (wd_hbm, wd_ref), (proj_hbm, proj_ref),
                (cin_hbm, cin_ref), (routes_hbm, routes_ref), (weight_hbm, weight_ref),
                (taps_hbm, taps_ref), (rmap_hbm, rmap_ref), (imap_hbm, imap_ref),
                (param_hbm, param_ref), (branch_hbm, branch_ref),
            )
        )
    ]
    for i in (8, 9, 0, 1, 7, 10, 11, 12, 13, 2, 14, 3, 4, 5, 6):
        loads[i].start()

    barrier, heard = announce(n, (partner, across))
    puts = []

    def store(src, dst):
        copy = pltpu.make_async_copy(src, dst, put.at[len(puts)])
        copy.start()
        puts.append(copy)

    loads[8].wait()
    loads[9].wait()
    route0, route1 = routes_ref[0:1], routes_ref[1:2]
    offset = lax.broadcasted_iota(jnp.int32, (n, length), 0)
    which = (offset + sp) % n if n & (n - 1) else offset ^ sp
    first, second = which == route0, which == route1
    named = (first | second).astype(F32).astype(BF)
    earlier = lax.broadcasted_iota(jnp.int32, (length, length), 0) < lax.broadcasted_iota(
        jnp.int32, (length, length), 1
    )
    rank = jnp.dot(named, earlier.astype(F32).astype(BF), preferred_element_type=F32)
    place = (offset * slots).astype(F32) + rank
    target0 = jnp.sum(jnp.where(first, place, 0.0), axis=0, keepdims=True).astype(jnp.int32)
    target1 = jnp.sum(jnp.where(second, place, 0.0), axis=0, keepdims=True).astype(jnp.int32)
    loads[0].wait()
    for r in range(0, length, 32):
        x = x_ref[r : r + 32].astype(F32)
        inv = lax.rsqrt(jnp.mean(x * x, axis=1, keepdims=True) + EPS)
        nx_ref[r : r + 32] = (x * inv).astype(BF)

    def chosen(lo, hi):
        slot = lax.broadcasted_iota(jnp.int32, ((hi - lo) * slots, length), 0) + lo * slots
        hit0, hit1 = slot == target0, slot == target1
        pick = (hit0 | hit1).astype(F32).astype(BF)
        pick_ref[lo * slots : hi * slots] = pick
        share = jnp.where(hit0, weight_ref[0:1], 0.0) + jnp.where(hit1, weight_ref[1:2], 0.0)
        return pick, jnp.sum(share, axis=1, keepdims=True)

    def taken(pick, share, where):
        cot = jnp.dot(pick, cot_ref[:, where], preferred_element_type=F32)
        got = jnp.dot(pick, nx_ref[:, where], preferred_element_type=F32).astype(BF)
        return (cot * share).astype(BF), got

    order = [
        d for lo, hi in ((1, 4 * unit), (6 * unit, n), (4 * unit, 6 * unit)) for d in range(lo, hi)
    ]
    hops = {}
    loads[1].wait()
    for lo, hi in ((0, 4 * unit), (4 * unit, n)):
        pick, share = chosen(lo, hi)
        for a, value in enumerate(taken(pick, share, cols(tp))):
            send_ref[a, lo:hi] = value.reshape(hi - lo, slots, fourth)
        if lo == 0:
            own = pick[:slots], share[:slots]
            pl.semaphore_wait(barrier, heard)
            loads[7].wait()
            edges = edge_copies(n, cin_ref, halo_ref, edge)
        for d in order:
            if lo <= d < hi:
                for a in range(2):
                    copy = remote(
                        send_ref.at[a, d], rows[a].at[d, :, cols(tp)], hop, (a, d),
                        (partner_at(sp, n, d), tp),
                    )
                    copy.start()
                    hops[a, d] = copy
    for q in range(width // fourth):
        where = pl.ds(q * fourth, fourth)
        rows_sc[0, :, where], rows_in[0, :, where] = taken(*own, where)

    for i in (10, 11, 12, 13):
        loads[i].wait()
    plus = softplus(-param_ref[...])
    heads, hw = rmap_ref.shape[1], rmap_ref.shape[2]
    spread = (
        lax.broadcasted_iota(jnp.int32, (hw, channels), 1) % hw
        == lax.broadcasted_iota(jnp.int32, (hw, channels), 0)
    ).astype(F32).astype(BF)
    block = (
        lax.broadcasted_iota(jnp.int32, (channels, channels), 0) // hw
        == lax.broadcasted_iota(jnp.int32, (channels, channels), 1) // hw
    )
    for i in range(4):
        stack = (rmap_ref, imap_ref)[i % 2][i // 2].reshape(heads * hw, hw)
        full = jnp.dot(stack, spread, preferred_element_type=F32)
        maps_ref[:, i * channels : (i + 1) * channels] = jnp.where(block, full, 0.0).astype(BF)
    for copy in edges:
        copy.wait()
    taps = taps_ref[...].astype(F32)
    low, high = halo_rows(halo_ref, n)
    x = cin_ref[...].astype(F32)
    back1 = shifted(x, 1, low[1:2])
    back2 = shifted(back1, 1, low[0:1])
    conv = back2 * taps[0:1] + back1 * taps[1:2] + x * taps[2:3]
    conv = conv + shifted(x, -1, high[0:1]) * taps[3:4]
    conv_ref[...] = conv
    gates_ref[...] = jax.nn.sigmoid(split_dot(conv, maps_ref[...], PLAIN))
    loads[2].wait()
    for d in range(2):
        recur = gates_ref[:, 2 * d * channels : (2 * d + 1) * channels]
        inputs = gates_ref[:, (2 * d + 1) * channels : (2 * d + 2) * channels]
        log_decay = -DECAY_SCALE * recur * plus[d : d + 1] + shift_ref[d]
        root = jnp.sqrt(minus_expm1(2.0 * log_decay))
        decay_ref[d] = jnp.exp(log_decay)
        root_ref[d] = root
        drive_ref[d] = root * (inputs * conv_ref[...])
    a_f, a_b = decay_ref.at[0], decay_ref.at[1]
    ends = run_scans(
        length,
        (
            (False, a_f, drive_ref.at[0], state_ref.at[0]),
            (True, a_b, drive_ref.at[1], state_ref.at[1]),
            (False, a_f, None, cum_ref.at[0]),
            (True, a_b, None, cum_ref.at[1]),
            (True, a_f, None, ones_ref.at[0]),
            (False, a_b, None, ones_ref.at[1]),
        ),
    )
    tot_ref[0:1, :] = ends[2]
    tot_ref[1:2, :] = ends[0]
    tot_ref[2:3, :] = ends[3]
    tot_ref[3:4, :] = ends[1]
    tot_ref[4:8, :] = jnp.zeros((4, channels), F32)
    totals = []
    for d in range(n - 1, 0, -1):
        copy = remote(tot_ref, all_ref.at[sp], s_tot, (d,), (partner_at(sp, n, d), tp))
        copy.start()
        totals.append(copy)
    all_ref[sp] = tot_ref[...]

    def finish_states():
        for copy in totals:
            copy.wait()
        in_f, in_b = carries(n, all_ref, ((0, 1), (2, 3)))
        state_f = state_ref[0] + cum_ref[0] * in_f
        state_b = state_ref[1] + cum_ref[1] * in_b
        beside = (shifted(state_f, 1, in_f), shifted(state_b, -1, in_b))
        loads[14].wait()
        value, slope = gelu_parts(branch_ref[...].astype(F32))
        states = state_f + state_b
        value_ref[...] = value
        slope_ref[...] = states * slope
        out_all[0] = (value * states).astype(BF)
        conv = conv_ref[...]
        for d in range(2):
            recur = gates_ref[:, 2 * d * channels : (2 * d + 1) * channels]
            inputs = gates_ref[:, (2 * d + 1) * channels : (2 * d + 2) * channels]
            decay = decay_ref[d]
            root = root_ref[d]
            a_ref[d] = root * inputs
            g_log = beside[d] * decay - inputs * conv * (decay * decay) / root
            c_ref[d] = g_log * (-DECAY_SCALE * plus[d : d + 1]) * recur * (1.0 - recur)
            e_ref[d] = root * conv * inputs * (1.0 - inputs)

    nears, fwds, overs, late = {}, {}, {}, []

    def step_in(a, d):
        hops[a, d].wait_recv()
        dst = rows[a]
        mine = dst.at[d, :, cols(tp)]
        overs[a, d] = remote(mine, mine, cross, (a, d), (sp, across))
        overs[a, d].start()
        late.append((a, d))
        nears[a, d] = remote(mine, mine, pair, (a, d), (sp, partner))
        nears[a, d].start()

    def step_on():
        a, d = late.pop(0)
        overs[a, d].wait_recv()
        other = rows[a].at[d, :, cols(across)]
        fwds[a, d] = remote(other, other, fwd, (a, d), (sp, partner))
        fwds[a, d].start()

    def bring(lo, hi):
        for d in order:
            if lo * unit <= d < hi * unit:
                for a in range(2):
                    step_in(a, d)
                    if len(late) > LAG:
                        step_on()

    pairs, crosses, backs = {}, {}, {}

    def experts(lo, hi):
        lo, hi = lo * unit, hi * unit
        while any(lo <= d < hi for _, d in late):
            step_on()
        for d in range(lo, hi):
            if d:
                for a in range(2):
                    nears[a, d].wait_recv()
                    fwds[a, d].wait_recv()
        count = (hi - lo) * slots
        at = slice(lo * slots, hi * slots)
        xin = rows_in[lo:hi].reshape(count, width)
        gate_pre = jnp.dot(xin, wg_ref[...], preferred_element_type=F32)
        up_pre = jnp.dot(xin, wu_ref[...], preferred_element_type=F32)
        xsc = rows_sc[lo:hi].reshape(count, width)
        hidden_grad = lax.dot_general(xsc, wd_ref[...], COLS1, preferred_element_type=F32)
        gate_sig = jax.nn.sigmoid(gate_pre)
        gate_act = gate_pre * gate_sig
        hid_ref[at] = (gate_act * up_pre).astype(BF)
        gate_grad = hidden_grad * up_pre * gate_sig * (1.0 + gate_pre * (1.0 - gate_sig))
        gate_grad = gate_grad.astype(BF)
        up_grad = (hidden_grad * gate_act).astype(BF)
        units = up_grad.shape[1]
        ggu_ref[at, :units] = gate_grad
        ggu_ref[at, units:] = up_grad
        for i, q in enumerate((diagonal, partner, across, tp)):
            some = pl.ds(pl.multiple_of(q * fourth, 128), fourth)
            total = lax.dot_general(gate_grad, wg_ref[some], COLS1, preferred_element_type=F32)
            total = total + lax.dot_general(up_grad, wu_ref[some], COLS1, preferred_element_type=F32)
            part_ref[lo:hi, :, cols(q)] = total.astype(BF).reshape(hi - lo, slots, fourth)
            if i < 2:
                for d in range(lo, hi):
                    copy = remote(
                        part_ref.at[d, :, cols(q)], got1.at[i, d], s_pair, (i, d), (sp, partner)
                    )
                    copy.start()
                    pairs[i, d] = copy

    def stage_b(lo, hi):
        for d in range(lo * unit, hi * unit):
            pairs[0, d].wait_recv()
            total = part_ref[d, :, cols(across)].astype(F32) + got1[0, d].astype(F32)
            mid[d] = total.astype(BF)
            crosses[d] = remote(mid.at[d], got2.at[d], s_cross, (d,), (sp, across))
            crosses[d].start()

    def stage_c(lo, hi):
        for d in range(lo * unit, hi * unit):
            pairs[1, d].wait_recv()
            crosses[d].wait_recv()
            total = part_ref[d, :, cols(tp)].astype(F32) + got1[1, d].astype(F32)
            total = (total + got2[d].astype(F32)).astype(BF)
            if d == 0:
                back[0] = total
            else:
                fin[d] = total
                backs[d] = remote(fin.at[d], back.at[d], s_hop, (d,), (source_at(sp, n, d), tp))
                backs[d].start()

    chunk = width // 8

    def weight_gradients(k):
        at = slice(k * chunk, (k + 1) * chunk)
        units = hid_ref.shape[1]
        left = rows_in[:, :, at].reshape(n * slots, chunk)
        both = lax.dot_general(left, ggu_ref[...], ROWS0, preferred_element_type=F32)
        ggate_ref[at] = both[:, :units]
        gup_ref[at] = both[:, units:]
        right = rows_sc[:, :, at].reshape(n * slots, chunk)
        gdown_ref[:, at] = lax.dot_general(hid_ref[...], right, ROWS0, preferred_element_type=F32)
        store(ggate_ref.at[at], ggate_hbm.at[at])
        store(gup_ref.at[at], gup_hbm.at[at])
        store(gdown_ref.at[:, at], gdown_hbm.at[:, at])

    powers = n & (n - 1) == 0
    bits = [n >> i for i in range(1, n.bit_length())] if powers else []
    gathers = []

    def gather(pairs_of):
        got = []
        for d, to, hop_to in pairs_of:
            copy = remote(out_all.at[d], out_all.at[to], s_out, (to,), (partner_at(sp, n, hop_to), tp))
            copy.start()
            got.append(copy)
        gathers.append(got)

    def gather_start():
        if powers:
            bit = bits.pop(0)
            gather([(d, d + bit, bit) for d in range(0, n, 2 * bit)])
        else:
            gather([(0, d, d) for d in range(1, n)])

    def gather_on():
        if bits:
            for copy in gathers[-1]:
                copy.wait_recv()
            gather_start()

    bring(0, 2)
    bring(2, 4)
    for i in (3, 4, 5):
        loads[i].wait()
    experts(0, 2)
    bring(6, 8)
    experts(2, 4)
    bring(4, 6)
    experts(6, 8)
    stage_b(6, 8)
    experts(4, 6)
    stage_c(6, 8)
    stage_b(4, 6)
    stage_b(2, 4)
    stage_c(4, 6)
    stage_b(0, 2)
    stage_c(2, 4)
    stage_c(0, 2)
    finish_states()
    weight_gradients(0)
    gather_start()
    for k in range(1, 8):
        weight_gradients(k)
    for d in range(1, n):
        backs[d].wait_recv()
    got = back[...].reshape(n * slots, fourth)
    grad = lax.dot_general(pick_ref[...], got, ROWS0, preferred_element_type=F32)
    ng_ref[:, cols(tp)] = grad.astype(BF)
    own = ng_ref.at[:, cols(tp)]
    half = length // 2
    overs_h, lasts = [], []
    for h in range(2):
        block = ng_ref.at[pl.ds(h * half, half), cols(tp)]
        overs_h.append(remote(block, block, s_tail, (h,), (sp, across)))
        overs_h[h].start()
    near = remote(own, own, s_tail, (2,), (sp, partner))
    near.start()
    for h in range(2):
        overs_h[h].wait_recv()
        block = ng_ref.at[pl.ds(h * half, half), cols(across)]
        lasts.append(remote(block, block, s_tail, (3 + h,), (sp, partner)))
        lasts[h].start()
    gather_on()
    for group in (hops, nears, fwds, overs, pairs, crosses, backs):
        for copy in group.values():
            copy.wait_send()
    near.wait()
    for copy in overs_h:
        copy.wait_send()

    part = width // n
    mine = pl.ds(pl.multiple_of((tp % 2) * half, ROW_TILE), half)
    for r in range(0, length, ROW_TILE):
        if r % half == 0:
            lasts[r // half].wait()
        x = x_ref[r : r + ROW_TILE].astype(F32)
        inv = lax.rsqrt(jnp.mean(x * x, axis=1, keepdims=True) + EPS)
        normed = x * inv
        ng = ng_ref[r : r + ROW_TILE].astype(F32)
        dot = jnp.mean(ng * normed, axis=1, keepdims=True)
        mixed = (cot_ref[r : r + ROW_TILE].astype(F32) + inv * (ng - normed * dot)).astype(BF)
        for e in range(n):
            mixed_ref[e, r : r + ROW_TILE] = mixed[:, e * part : (e + 1) * part]
    mixes, shares = {}, {}

    def mix(ds):
        for d in ds:
            peer = partner_at(sp, n, d)
            mixes[d] = remote(
                mixed_ref.at[peer, mine], mixed_all.at[d, mine], s_mix, (d,), (peer, tp)
            )
            mixes[d].start()

    reach = order[::-1]
    early = []
    mix(early)
    loads[6].wait()
    out_grad = jnp.zeros((length, channels), F32)
    for e in range(n):
        out_grad = out_grad + jnp.dot(
            mixed_ref[e], proj_ref[e * part : (e + 1) * part], preferred_element_type=F32
        )
    carried = out_grad * value_ref[...]
    branch_grad_ref[...] = (out_grad * slope_ref[...]).astype(BF)
    store(branch_grad_ref, branch_grad_hbm)
    drive_ref[...] = decay_ref[...] * carried[None]
    ends = run_scans(
        length,
        (
            (True, decay_ref.at[0], drive_ref.at[0], after_ref.at[0]),
            (False, decay_ref.at[1], drive_ref.at[1], after_ref.at[1]),
        ),
    )
    msg_ref[0:1, :] = tot_ref[0:1, :]
    msg_ref[1:2, :] = tot_ref[2:3, :]
    msg_ref[2:3, :] = ends[1]
    msg_ref[3:4, :] = ends[0]
    msg_ref[4:8, :] = jnp.zeros((4, channels), F32)
    sums = []
    for d in range(n - 1, 0, -1):
        copy = remote(msg_ref, every_ref.at[sp], s_msg, (d,), (partner_at(sp, n, d), tp))
        copy.start()
        sums.append(copy)
    every_ref[sp] = msg_ref[...]
    mix([d for d in reach if d not in early])
    mixed_all[0] = mixed_ref[sp]
    gather_on()
    for copy in sums:
        copy.wait()
    in_ab, in_af = carries(n, every_ref, ((1, 2), (0, 3)))
    after_f = after_ref[0] + ones_ref[0] * in_af
    after_b = after_ref[1] + ones_ref[1] * in_ab
    adjoint = (carried + shifted(after_f, -1, in_af), carried + shifted(after_b, 1, in_ab))
    total = adjoint[0] * a_ref[0] + adjoint[1] * a_ref[1]
    for d in range(2):
        gates_ref[:, 2 * d * channels : (2 * d + 1) * channels] = adjoint[d] * c_ref[d]
        gates_ref[:, (2 * d + 1) * channels : (2 * d + 2) * channels] = adjoint[d] * e_ref[d]
    total = total + split_dot(gates_ref[...], maps_ref[...], COLS1)
    conv_grad_ref[...] = total.astype(BF)
    rims = edge_copies(n, conv_grad_ref, halo2_ref, s_edge)
    while bits:
        gather_on()
    for d in reach:
        mixes[d].wait_recv()
        block = mixed_all.at[d, mine]
        shares[d] = remote(block, block, s_share, (d,), (sp, partner))
        shares[d].start()
    for copy in rims:
        copy.wait()
    taps = taps_ref[...].astype(F32)
    low, high = halo_rows(halo2_ref, n)
    up1 = shifted(total, -1, high[0:1])
    up2 = shifted(up1, -1, high[1:2])
    down = shifted(total, 1, low[1:2])
    result = up2 * taps[0:1] + up1 * taps[1:2] + total * taps[2:3] + down * taps[3:4]
    input_grad_ref[...] = result.astype(BF)
    store(input_grad_ref, input_grad_hbm)
    for d in range(1, n):
        shares[d].wait()
        mixes[d].wait_send()
    for got in gathers[:-1]:
        for copy in got:
            copy.wait_send()
    for copy in gathers[-1]:
        copy.wait()
    grad_out_ref[...] = lax.dot_general(
        mixed_all[...].reshape(n * length, part),
        out_all[...].reshape(n * length, channels),
        ROWS0,
        preferred_element_type=F32,
    )
    store(grad_out_ref, grad_out_hbm)
    for copy in puts:
        copy.wait()


def whole(args, n, n_tp, slots):
    cot, wg, proj, cin = args[0], args[4], args[7], args[8]
    length, width = cot.shape
    channels = cin.shape[1]
    units = wg.shape[1]
    fourth = width // n_tp
    part = width // n
    dma = pltpu.SemaphoreType.DMA
    sds = jax.ShapeDtypeStruct
    vm = pltpu.VMEM
    one, two = (length, channels), (2, length, channels)
    outs = (
        sds((width, units), F32),
        sds((width, units), F32),
        sds((units, width), F32),
        sds((part, channels), F32),
        sds(one, BF),
        sds(one, BF),
    )
    block = (n, slots, fourth)
    scratch = [
        *(vm(args[i].shape, args[i].dtype) for i in (2, 3, 8, 9, 10, 11, 12, 13)),
        vm((length, width), BF), vm((length, width), BF), vm((length, width), BF),
        vm((width, units), BF), vm((width, units), BF), vm((units, width), BF),
        vm(proj.shape, BF), vm(two, F32),
        vm((length, width), BF),
        *(vm(out.shape, out.dtype) for out in outs),
        vm((n * slots, length), BF), vm((2,) + block, BF),
        vm((n, slots, width), BF), vm((n, slots, width), BF),
        vm((n * slots, units), BF), vm((n * slots, 2 * units), BF), vm((n, slots, width), BF),
        vm((2,) + block, BF), vm(block, BF), vm(block, BF), vm(block, BF), vm(block, BF),
        vm((2, ROW_TILE, channels), BF),
        vm((channels, 4 * channels), BF),
        vm(two, F32), vm(two, F32), vm(two, F32), vm(two, F32), vm(two, F32),
        vm(one, F32), vm(one, F32), vm((8, channels), F32),
        vm(one, F32), vm((length, 4 * channels), F32), vm(two, F32), vm(two, F32), vm(two, F32),
        vm(two, F32), vm((n, 8, channels), F32),
        vm((n, length, part), BF), vm((n, length, part), BF), vm((n, length, channels), BF),
        vm(two, F32), vm((8, channels), F32), vm((n, 8, channels), F32),
        vm((length, channels), BF), vm((2, ROW_TILE, channels), BF),
        dma((15,)), dma((3 * 8 + 3,)),
        dma((2, 2)), dma((2, 2, n)), dma((2, 2, n)), dma((2, 2, n)),
        dma((2, 2, n)), dma((2, 2, n)), dma((2, n)), dma((2, n)), dma((2, 5)), dma((2, n)),
        dma((2, n)), dma((2, n)), dma((2, n)), dma((2, n)), dma((2, 2)),
    ]
    return pl.pallas_call(
        functools.partial(whole_kernel, n, slots),
        out_shape=outs,
        in_specs=[HB] * len(args),
        out_specs=[HB] * len(outs),
        scratch_shapes=scratch,
        compiler_params=pltpu.CompilerParams(
            collective_id=1, has_side_effects=True, vmem_limit_bytes=VMEM_LIMIT
        ),
        cost_estimate=pl.CostEstimate(
            flops=2_000_000_000, bytes_accessed=30_000_000, transcendentals=0
        ),
    )(*args)


def written(*arrays):
    count = len(arrays)
    cuts = [4 if x.size * x.dtype.itemsize > 2**20 else 1 for x in arrays]
    offsets = [sum(cuts[:i]) for i in range(count)]

    def kernel(*refs):
        sems = refs[-1]
        sets = []
        for i in range(count):
            src, dst, held = refs[i], refs[count + i], refs[2 * count + i]
            step = src.shape[0] // cuts[i]
            for k in range(cuts[i]):
                at = pl.ds(k * step, step)
                j = offsets[i] + k
                inward = pltpu.make_async_copy(src.at[at], held.at[at], sems.at[0, j])
                outward = pltpu.make_async_copy(held.at[at], dst.at[at], sems.at[1, j])
                inward.start()
                sets.append((inward, outward))
        for inward, outward in sets:
            inward.wait()
            outward.start()
        for _, outward in sets:
            outward.wait()

    return pl.pallas_call(
        kernel,
        out_shape=tuple(jax.ShapeDtypeStruct(x.shape, x.dtype) for x in arrays),
        in_specs=[HB] * count,
        out_specs=[HB] * count,
        scratch_shapes=[pltpu.VMEM(x.shape, x.dtype) for x in arrays]
        + [pltpu.SemaphoreType.DMA((2, sum(cuts)))],
        compiler_params=pltpu.CompilerParams(vmem_limit_bytes=VMEM_LIMIT),
    )(*arrays)


def shards(
    cotangent,
    saved_input,
    routes,
    route_weight,
    gate_proj,
    up_proj,
    down_proj,
    out_proj,
    conv_input,
    gate_branch,
    conv_taps,
    recur_map,
    input_map,
    decay_param,
    decay_shift,
):
    length, _ = cotangent.shape
    n = lax.axis_size("sp")
    n_tp = lax.axis_size("tp")
    slots = 4 * length // n
    slots = (slots + ROW_TILE - 1) // ROW_TILE * ROW_TILE
    grad_gate, grad_up, grad_down, *others = written(
        *whole(
            (
                cotangent, saved_input, routes.T, route_weight.T, gate_proj[0], up_proj[0],
                down_proj[0], out_proj, conv_input, gate_branch, conv_taps, recur_map, input_map,
                decay_param, decay_shift,
            ),
            n, n_tp, slots,
        )
    )
    return (grad_gate[None], grad_up[None], grad_down[None], *others)


def solution(mesh):
    in_specs = (
        P("sp", None),
        P("sp", None),
        P("sp", None),
        P("sp", None),
        P("sp", None, "tp"),
        P("sp", None, "tp"),
        P("sp", "tp", None),
        P(None, "tp"),
        P("sp", "tp"),
        P("sp", "tp"),
        P(None, "tp"),
        P(None, "tp", None, None),
        P(None, "tp", None, None),
        P(None, "tp"),
        P(None, "sp", "tp"),
    )
    out_specs = (
        P("sp", None, "tp"),
        P("sp", None, "tp"),
        P("sp", "tp", None),
        P("sp", "tp"),
        P("sp", "tp"),
        P("sp", "tp"),
    )
    return jax.shard_map(shards, mesh=mesh, in_specs=in_specs, out_specs=out_specs, check_vma=False)
```
